256 devices in a mesh: fs: 32 (over z, x), tp: 8 (over y, core).
Axes of the slice: x: 4, y: 4, z: 8, core: 2. Of those that a mesh axis runs over, the one named last changes fastest.
Arguments:
- later_rows: bfloat16 [32768, 2048], P(('fs', 'tp')), may hold values from -6 to 6
- earlier_rows: bfloat16 [32768, 2048], P(('fs', 'tp')), may hold values from -6 to 6
- cotangent: bfloat16 [32768, 2048], P(('fs', 'tp')), may hold values from -24 to 24
- up_weight: bfloat16 [2048, 4096], P('fs', 'tp'), may hold values from -0.125 to 0.125
- down_weight: bfloat16 [2048, 4096], P('fs', 'tp'), may hold values from -0.09375 to 0.09375
- up_total: float32 [2048, 4096], P('fs', 'tp'), may hold values from -6 to 6
- down_total: float32 [2048, 4096], P('fs', 'tp'), may hold values from -6 to 6
Outputs:
- later_out: bfloat16 [32768, 2048], P(('fs', 'tp'))
- earlier_grad: bfloat16 [32768, 2048], P(('fs', 'tp'))
- up_updated: float32 [2048, 4096], P('fs', 'tp')
- down_updated: float32 [2048, 4096], P('fs', 'tp')
The draws below stay inside these ranges and needn't reach their ends.
All inputs are finite; a program needn't handle non-finite values.
Results may differ from the reference program's by a relative error of at most 0.015.
Values may be sent and summed in bfloat16 or wider, within the bound.
No kernel may reach another device: no remote copies, remote signals or barrier semaphores. Data moves between devices by JAX's collectives and lax.ppermute only.
A program may use at most 128 MiB of HBM per device.

```python
import math
import jax
import jax.numpy as jnp
from jax import lax

D = 2048
FF = 4096
TOKENS = 32768
FF_TP = 512
N_TP = 8


def spiked(drawn, rng, source, target, shards_of, factor):
    def block_of(position):
        return (jnp.arange(drawn.shape[position]) // (drawn.shape[position] // shards_of)).reshape((-1,) + (1,) * (drawn.ndim - 1 - position))

    one_side = jax.random.permutation(rng, shards_of)[block_of(target)]
    far = (block_of(target) + shards_of // 2) % shards_of
    return jnp.where((block_of(source) == one_side) | (block_of(source) == far), factor * drawn, drawn)


def steps_of(rng, dims, split, low, largest):
    def one(axis_at, parts):
        steps = jax.random.uniform(jax.random.fold_in(jax.random.fold_in(rng, 6), axis_at), (parts,), jnp.float32, low / len(split), largest / len(split))
        return jnp.repeat(jnp.exp(steps), dims[axis_at] // parts).reshape((-1,) + (1,) * (len(dims) - axis_at - 1))

    level = one(*split[0])
    for cut in split[1:]:
        level = level * one(*cut)
    return level


def scatter_about(key, extent, width, reach, shards=(), kind=jnp.bfloat16):
    loudness = steps_of(key, extent, shards, -0.22, 0.18) if shards else 1.0
    array = jax.random.normal(key, extent, jnp.float32) * width * loudness
    return jnp.minimum(jnp.maximum(array, -reach), reach).astype(kind)


def noise_with(stream_key, dims, width, reach, shards, heavy, kind=jnp.bfloat16):
    entries = width * jax.random.normal(stream_key, dims, jnp.float32)
    if shards:
        entries = entries * steps_of(stream_key, dims, shards, -0.22, 0.18)
    return jnp.clip(spiked(entries, jax.random.fold_in(stream_key, 3), *heavy), -reach, reach).astype(kind)


def setup_inputs(seed: int = 0) -> dict:
    keys = jax.random.split(jax.random.key(seed), 8)
    return {
        "later_rows": scatter_about(keys[0], (TOKENS, D), 1.0, 6.0, ((0, 256),)),
        "earlier_rows": scatter_about(keys[1], (TOKENS, D), 1.0, 6.0, ((0, 256),)),
        "cotangent": noise_with(keys[2], (TOKENS, D), 1.0, 24.0, ((0, 256),), (0, 1, 256, 6.0)),
        "up_weight": scatter_about(keys[3], (D, FF), D ** -0.5, 0.125, ((0, 32), (1, 8))),
        "down_weight": scatter_about(keys[4], (D, FF), FF ** -0.5, 0.09375, ((0, 32), (1, 8))),
        "up_total": scatter_about(keys[5], (D, FF), 1.0, 6.0, ((0, 32), (1, 8)), jnp.float32),
        "down_total": scatter_about(keys[6], (D, FF), 1.0, 6.0, ((0, 32), (1, 8)), jnp.float32),
    }


def blocked_sum(left, right):

    def one_block(carry, index):
        start = (index * FF_TP).astype(jnp.int32)
        left_block = lax.dynamic_slice_in_dim(left, start, FF_TP, 1)
        right_block = lax.dynamic_slice_in_dim(right, start, FF_TP, 1)
        partial_value = lax.dot_general(left_block, right_block, (((1,), (1,)), ((), ())), preferred_element_type=jnp.float32)
        rounded = lax.optimization_barrier(partial_value.astype(jnp.bfloat16))
        return (carry + rounded.astype(jnp.float32), None)
    init = jnp.zeros((left.shape[0], right.shape[0]), jnp.float32)
    total, _ = lax.scan(one_block, init, jnp.arange(N_TP, dtype=jnp.int32))
    return total

def reference(later_rows, earlier_rows, cotangent, up_weight, down_weight, up_total, down_total):
    later_pre = jnp.dot(later_rows, up_weight, preferred_element_type=jnp.float32)
    later_relu = jnp.maximum(later_pre, 0.0)
    later_hidden = (later_relu * later_relu).astype(jnp.bfloat16)
    later_out = blocked_sum(later_hidden, down_weight).astype(jnp.bfloat16)
    earlier_pre = jnp.dot(earlier_rows, up_weight, preferred_element_type=jnp.float32)
    earlier_relu = jnp.maximum(earlier_pre, 0.0)
    earlier_hidden = (earlier_relu * earlier_relu).astype(jnp.bfloat16)
    hidden_grad = jnp.dot(cotangent, down_weight, preferred_element_type=jnp.float32)
    pre_grad = (2.0 * earlier_relu * hidden_grad).astype(jnp.bfloat16)
    earlier_grad = blocked_sum(pre_grad, up_weight).astype(jnp.bfloat16)
    factor = 1.0 / math.sqrt(TOKENS)
    up_term = jnp.dot(earlier_rows.T, pre_grad, preferred_element_type=jnp.float32)
    down_term = jnp.dot(cotangent.T, earlier_hidden, preferred_element_type=jnp.float32)
    up_updated = up_total + up_term * factor
    down_updated = down_total + down_term * factor
    return (later_out, earlier_grad, up_updated, down_updated)
```

```python
import math

import jax
import jax.numpy as jnp
from jax import lax
from jax.sharding import Mesh
from jax.sharding import PartitionSpec as P

FS = ("z", "x")
ALL = ("z", "x", "y", "c")
F32 = jnp.float32
BF16 = jnp.bfloat16


def shift(x, axis, by):
    n = lax.axis_size(axis)
    return lax.ppermute(x, axis, [(i, (i + by) % n) for i in range(n)])


def gather_tokens(x):
    half = x.shape[0] // 2
    behind, ahead = shift(x, "y", 1), shift(x, "y", -1)
    far_lo, far_hi = shift(behind[:half], "y", 1), shift(ahead[half:], "y", -1)
    mine = jnp.concatenate([x, behind, ahead, far_lo, far_hi], axis=0)
    return jnp.concatenate([mine, shift(mine, "c", 1)], axis=0)


def plus(a, b):
    return (a.astype(F32) + b.astype(F32)).astype(BF16)


def scatter_tokens(partial):
    mine, partners = jnp.split(partial, 2, axis=0)
    mine = plus(mine, shift(partners, "c", 1))
    rows = mine.shape[0] // 4
    half = rows // 2
    own, behind, ahead, far = (mine[i * rows : (i + 1) * rows] for i in range(4))
    from_behind = shift(far[:half], "y", 1)
    from_ahead = shift(far[half:], "y", -1)
    ahead = jnp.concatenate([plus(ahead[:half], from_behind), ahead[half:]], axis=0)
    behind = jnp.concatenate([behind[:half], plus(behind[half:], from_ahead)], axis=0)
    a, b = shift(ahead, "y", 1), shift(behind, "y", -1)
    return (own.astype(F32) + a.astype(F32) + b.astype(F32)).astype(BF16)


def exchange_sum(term, axis, dim):
    tiles = lax.all_to_all(term, axis, dim, dim, tiled=True)
    return jnp.sum(tiles.astype(F32), axis=dim)


def rows_times(left, right):
    return lax.dot_general(left, right, (((1,), (1,)), ((), ())), preferred_element_type=F32)


def over_tokens(left, right):
    return lax.dot_general(left, right, (((0,), (0,)), ((), ())), preferred_element_type=F32)


def body(later_rows, earlier_rows, cotangent, up_weight, down_weight, up_total, down_total):
    n_dev = math.prod(lax.axis_size(a) for a in ALL)
    factor = 1.0 / math.sqrt(later_rows.shape[0] * n_dev)
    up = lax.all_gather(up_weight, FS, axis=0, tiled=True)
    down = lax.all_gather(down_weight, FS, axis=0, tiled=True)
    saved = gather_tokens(earlier_rows)
    cot = gather_tokens(cotangent)
    later = gather_tokens(later_rows)

    relu = jnp.maximum(jnp.dot(saved, up, preferred_element_type=F32), 0.0)
    hidden = (relu * relu).astype(BF16)
    down_term = over_tokens(cot, hidden).astype(BF16)
    down_term = lax.psum_scatter(down_term, "z", scatter_dimension=0, tiled=True)
    down_term = lax.psum_scatter(down_term, "x", scatter_dimension=0, tiled=True)
    later_relu = jnp.maximum(jnp.dot(later, up, preferred_element_type=F32), 0.0)
    later_hidden = (later_relu * later_relu).astype(BF16)

    hidden_grad = jnp.dot(cot, down, preferred_element_type=F32)
    pre_grad = (2.0 * relu * hidden_grad).astype(BF16)
    up_term = over_tokens(saved, pre_grad).astype(BF16)
    nz, nx = lax.axis_size("z"), lax.axis_size("x")
    up_term = up_term.reshape(nz, nx, up_weight.shape[0], up_weight.shape[1])
    up_term = exchange_sum(up_term, "x", 1).astype(BF16)
    up_term = exchange_sum(up_term, "z", 0)

    later_out = scatter_tokens(rows_times(later_hidden, down).astype(BF16))
    earlier_grad = scatter_tokens(rows_times(pre_grad, up).astype(BF16))
    up_updated = up_total + up_term * factor
    down_updated = down_total + down_term.astype(F32) * factor
    return later_out, earlier_grad, up_updated, down_updated


def solution(mesh):
    n_tp = mesh.shape["tp"]
    finer = Mesh(mesh.devices.reshape(8, 4, n_tp // 2, 2), ALL)
    rows, weight = P(ALL, None), P(FS, ("y", "c"))
    return jax.shard_map(
        body,
        mesh=finer,
        in_specs=(rows, rows, rows, weight, weight, weight, weight),
        out_specs=(rows, rows, weight, weight),
        check_vma=False,
    )
```

```python
import math

import jax
import jax.numpy as jnp
from jax import lax
from jax.sharding import Mesh
from jax.sharding import PartitionSpec as P


FS = ("z", "x")
ALL = ("z", "x", "y", "c")
F32 = jnp.float32
BF16 = jnp.bfloat16


def shift(x, axis, by):
    n = lax.axis_size(axis)
    return lax.ppermute(x, axis, [(i, (i + by) % n) for i in range(n)])


def place(buffer, piece, slot, row):
    return lax.dynamic_update_slice(buffer, piece[:, None], (0, slot, row, 0))


def gather_tokens(arrays):
    own = jnp.stack(arrays)
    half = own.shape[1] // 2
    behind, ahead = shift(own, "y", 1), shift(own, "y", -1)
    far_lo, far_hi = shift(behind[:, :half], "y", 1), shift(ahead[:, half:], "y", -1)
    group = jnp.zeros((own.shape[0], 8, *own.shape[1:]), BF16)
    for piece, slot, row in (
        (own, 0, 0), (behind, 1, 0), (ahead, 2, 0), (far_lo, 3, 0), (far_hi, 3, half)
    ):
        partners = shift(piece, "c", 1)
        group = place(place(group, piece, slot, row), partners, slot + 4, row)
    return tuple(g.reshape(-1, g.shape[-1]) for g in group)


def plus(a, b):
    return (a.astype(F32) + b.astype(F32)).astype(BF16)


def scatter_tokens(partial):
    mine, partners = jnp.split(partial, 2, axis=0)
    partners = shift(partners, "c", 1)
    mine = plus(mine, partners)
    rows = mine.shape[0] // 4
    half = rows // 2
    own, behind, ahead, far = (mine[i * rows : (i + 1) * rows] for i in range(4))
    from_behind = shift(far[:half], "y", 1)
    from_ahead = shift(far[half:], "y", -1)
    ahead = jnp.concatenate([plus(ahead[:half], from_behind), ahead[half:]], axis=0)
    behind = jnp.concatenate([behind[:half], plus(behind[half:], from_ahead)], axis=0)
    a, b = shift(ahead, "y", 1), shift(behind, "y", -1)
    return (own.astype(F32) + a.astype(F32) + b.astype(F32)).astype(BF16)


def gather(x, axis):
    n = lax.axis_size(axis)
    return lax.all_to_all(jnp.broadcast_to(x[None], (n, *x.shape)), axis, 0, 0, tiled=True)


def exchange_sum(term, axis, dim):
    tiles = lax.all_to_all(term, axis, dim, dim, tiled=True)
    return jnp.sum(tiles.astype(F32), axis=dim)


def dot(left, right):
    return jnp.dot(left, right, preferred_element_type=F32)


def rows_times(left, right):
    return lax.dot_general(left, right, (((1,), (1,)), ((), ())), preferred_element_type=F32)


def over_tokens(left, right):
    return lax.dot_general(left, right, (((0,), (0,)), ((), ())), preferred_element_type=F32)


def body(later_rows, earlier_rows, cotangent, up_weight, down_weight, up_total, down_total):
    n_dev = math.prod(lax.axis_size(a) for a in ALL)
    nz, nx = lax.axis_size("z"), lax.axis_size("x")
    factor = 1.0 / math.sqrt(later_rows.shape[0] * n_dev)
    cols = up_weight.shape[1]
    up = gather(up_weight, "x").reshape(-1, cols)
    up = lax.all_gather(up, "z", axis=0, tiled=True)
    down = gather(down_weight, "z")
    down = gather(down, "x")
    down = jnp.swapaxes(down, 0, 1).reshape(-1, cols)
    saved, cot, later = gather_tokens((earlier_rows, cotangent, later_rows))

    relu = jnp.maximum(dot(saved, up), 0.0)
    hidden = (relu * relu).astype(BF16)
    down_term = over_tokens(cot, hidden).astype(BF16)
    down_term = lax.psum_scatter(down_term, "z", scatter_dimension=0, tiled=True)
    down_term = exchange_sum(down_term.reshape(-1, *down_weight.shape), "x", 0)
    hidden_grad = dot(cot, down)
    pre_grad = (2.0 * relu * hidden_grad).astype(BF16)
    up_term = over_tokens(saved, pre_grad).astype(BF16)
    up_term = up_term.reshape(nz, nx, *up_weight.shape)
    up_term = exchange_sum(up_term, "x", 1).astype(BF16)
    up_term = exchange_sum(up_term, "z", 0)
    later_relu = jnp.maximum(dot(later, up), 0.0)
    later_hidden = (later_relu * later_relu).astype(BF16)
    later_out = rows_times(later_hidden, down).astype(BF16)
    later_out = scatter_tokens(later_out)
    earlier_grad = rows_times(pre_grad, up).astype(BF16)
    earlier_grad = scatter_tokens(earlier_grad)
    up_updated = up_total + up_term * factor
    down_updated = down_total + down_term * factor
    return later_out, earlier_grad, up_updated, down_updated


def solution(mesh):
    n_tp = mesh.shape["tp"]
    finer = Mesh(mesh.devices.reshape(8, 4, n_tp // 2, 2), ALL)
    rows, weight = P(ALL, None), P(FS, ("y", "c"))
    return jax.shard_map(
        body,
        mesh=finer,
        in_specs=(rows, rows, rows, weight, weight, weight, weight),
        out_specs=(rows, rows, weight, weight),
        check_vma=False,
    )
```

```python
import math

import jax
import jax.numpy as jnp
from jax import lax
from jax.experimental import pallas as pl
from jax.experimental.pallas import tpu as pltpu
from jax.sharding import Mesh
from jax.sharding import PartitionSpec as P


FS = ("z", "x")
ALL = ("z", "x", "y", "c")
F32 = jnp.float32
BF16 = jnp.bfloat16
TILE = 512


def shift(x, axis, by):
    n = lax.axis_size(axis)
    return lax.ppermute(x, axis, [(i, (i + by) % n) for i in range(n)])


def gather_tokens(arrays):
    own = jnp.stack(arrays)
    half = own.shape[1] // 2
    behind, ahead = shift(own, "y", 1), shift(own, "y", -1)
    far_lo, far_hi = shift(behind[:, :half], "y", 1), shift(ahead[:, half:], "y", -1)
    pieces = (own, behind, ahead, far_lo, far_hi)
    partners = []
    for piece in pieces:
        partners.append(shift(piece, "c", 1))
    return (*pieces, *partners)


def plus(a, b):
    return (a.astype(F32) + b.astype(F32)).astype(BF16)


def scatter_tokens(mine, partners):
    partners = shift(partners, "c", 1)
    mine = plus(mine, partners)
    rows = mine.shape[0] // 4
    half = rows // 2
    own, behind, ahead, far = (mine[i * rows : (i + 1) * rows] for i in range(4))
    from_behind = shift(far[:half], "y", 1)
    from_ahead = shift(far[half:], "y", -1)
    ahead = jnp.concatenate([plus(ahead[:half], from_behind), ahead[half:]], axis=0)
    behind = jnp.concatenate([behind[:half], plus(behind[half:], from_ahead)], axis=0)
    a, b = shift(ahead, "y", 1), shift(behind, "y", -1)
    return (own.astype(F32) + a.astype(F32) + b.astype(F32)).astype(BF16)


def gather(x, axis):
    n = lax.axis_size(axis)
    return lax.all_to_all(jnp.broadcast_to(x[None], (n, *x.shape)), axis, 0, 0, tiled=True)


def exchange_sum(term, axis):
    tiles = lax.all_to_all(term, axis, 0, 0, tiled=True)
    return jnp.sum(tiles.astype(F32), axis=0)


def hop_sum(term, axis):
    n = lax.axis_size(axis)
    me = lax.axis_index(axis)

    def block(by):
        at = lax.rem(me + by, n)
        start = (at, *(0 for _ in term.shape[1:]))
        part = lax.dynamic_slice(term, start, (1, *term.shape[1:]), allow_negative_indices=False)
        return part[0]

    arrived = [shift(block(by), axis, by) for by in range(1, n)]
    return sum((a.astype(F32) for a in arrived), block(0).astype(F32))


def rows_times(left, right):
    return lax.dot_general(left, right, (((1,), (1,)), ((), ())), preferred_element_type=F32)


def over_tokens(left, right):
    return lax.dot_general(left, right, (((0,), (0,)), ((), ())), preferred_element_type=F32)


def copies(sources, target, sems, index):
    waits, row = [], 0
    for i, source in enumerate(sources):
        rows = source.shape[1]
        copy = pltpu.make_async_copy(source.at[index], target.at[pl.ds(row, rows)], sems.at[i])
        copy.start()
        waits.append((row, copy))
        row += rows
    return waits


def settle(waits, upto):
    while waits and waits[0][0] < upto:
        waits.pop(0)[1].wait()


def relu_times(rows, weight):
    return jnp.maximum(jnp.dot(rows, weight, preferred_element_type=F32), 0.0)


def back_kernel(*refs):
    pieces, (w, down_out, up_out, mine_out, theirs_out) = refs[:10], refs[10:15]
    saved, cot, up, down, relu, hid, pg, dt, ut, mine, theirs, in_sems, w_sems, out_sems = refs[15:]
    cols = up.shape[1]
    up_copy = pltpu.make_async_copy(w.at[:, pl.ds(0, cols)], up, w_sems.at[0])
    up_copy.start()
    saved_waits = copies(pieces, saved, in_sems.at[0], 0)
    down_copy = pltpu.make_async_copy(w.at[:, pl.ds(cols, cols)], down, w_sems.at[1])
    down_copy.start()
    cot_waits = copies(pieces, cot, in_sems.at[1], 1)
    up_copy.wait()
    for t in range(0, saved.shape[0], TILE):
        settle(saved_waits, t + TILE)
        at = pl.ds(t, TILE)
        r = relu_times(saved[at], up[...])
        relu[at] = r
        hid[at] = (r * r).astype(BF16)
    down_copy.wait()
    for t in range(0, saved.shape[0], TILE):
        settle(cot_waits, t + TILE)
        at = pl.ds(t, TILE)
        grad = jnp.dot(cot[at], down[...], preferred_element_type=F32)
        pg[at] = (2.0 * relu[at] * grad).astype(BF16)
    nx, nz, part = ut.shape[:3]

    @pl.loop(0, nz)
    def _(i):
        at = pl.ds(pl.multiple_of(i * nx * part, nx * part), nx * part)
        dt[at] = over_tokens(cot[:, at], hid[...]).astype(BF16)

    @pl.loop(0, nz)
    def _(i):
        at = pl.ds(pl.multiple_of(i * nx * part, nx * part), nx * part)
        term = over_tokens(saved[:, at], pg[...]).astype(BF16)
        for j in range(nx):
            ut[j, i] = term[j * part : (j + 1) * part]

    done = [
        pltpu.make_async_copy(a, b, out_sems.at[i])
        for i, (a, b) in enumerate(
            ((dt, down_out), (ut, up_out), (mine, mine_out), (theirs, theirs_out))
        )
    ]
    done[0].start()
    outputs(pg, 0, up, mine)
    done[1].start()
    outputs(pg, mine.shape[0], up, theirs)
    done[2].start()
    done[3].start()
    for copy in done:
        copy.wait()


def outputs(hidden, first, weight, out):
    @pl.loop(0, out.shape[0], step=TILE)
    def _(t):
        rows = hidden[pl.ds(pl.multiple_of(first + t, TILE), TILE)]
        for n in range(0, out.shape[1], 512):
            part = rows_times(rows, weight[n : n + 512])
            out[pl.ds(pl.multiple_of(t, TILE), TILE), n : n + 512] = part.astype(BF16)


def ahead_kernel(*refs):
    pieces, (w, mine_out, theirs_out) = refs[:10], refs[10:13]
    rows, up, down, hid, mine, theirs, in_sems, w_sems, out_sems = refs[13:]
    cols = up.shape[1]
    up_copy = pltpu.make_async_copy(w.at[:, pl.ds(0, cols)], up, w_sems.at[0])
    up_copy.start()
    waits = copies(pieces, rows, in_sems, 2)
    down_copy = pltpu.make_async_copy(w.at[:, pl.ds(cols, cols)], down, w_sems.at[1])
    down_copy.start()
    up_copy.wait()
    for t in range(0, rows.shape[0], TILE):
        settle(waits, t + TILE)
        at = pl.ds(t, TILE)
        r = relu_times(rows[at], up[...])
        hid[at] = (r * r).astype(BF16)
    down_copy.wait()
    first = pltpu.make_async_copy(mine, mine_out, out_sems.at[0])
    second = pltpu.make_async_copy(theirs, theirs_out, out_sems.at[1])
    outputs(hid, mine.shape[0], down, theirs)
    outputs(hid, 0, down, mine)
    second.start()
    first.start()
    first.wait()
    second.wait()


def call(kernel, pieces, weights, outs, scratch, dots):
    rows = sum(p.shape[1] for p in pieces)
    depth, cols = weights.shape[0], weights.shape[1] // 2
    hbm = pl.BlockSpec(memory_space=pltpu.HBM)
    return pl.pallas_call(
        kernel,
        out_shape=[jax.ShapeDtypeStruct(s, BF16) for s in outs],
        in_specs=[hbm] * (len(pieces) + 1),
        out_specs=[hbm] * len(outs),
        scratch_shapes=scratch,
        cost_estimate=pl.CostEstimate(
            flops=2 * dots * rows * depth * cols, bytes_accessed=20 << 20, transcendentals=0
        ),
        compiler_params=pltpu.CompilerParams(vmem_limit_bytes=60 * 1024 * 1024),
    )(*pieces, weights)


def back(pieces, weights, nz, nx):
    rows = sum(p.shape[1] for p in pieces)
    depth, cols = weights.shape[0], weights.shape[1] // 2
    n = len(pieces)
    up_shape = (nx, nz, depth // (nx * nz), cols)
    half = (rows // 2, depth)
    outs = ((depth, cols), up_shape, half, half)
    scratch = [
        pltpu.VMEM((rows, depth), BF16),
        pltpu.VMEM((rows, depth), BF16),
        pltpu.VMEM((depth, cols), BF16),
        pltpu.VMEM((depth, cols), BF16),
        pltpu.VMEM((rows, cols), F32),
        pltpu.VMEM((rows, cols), BF16),
        pltpu.VMEM((rows, cols), BF16),
        *(pltpu.VMEM(s, BF16) for s in outs),
        pltpu.SemaphoreType.DMA((2, n)),
        pltpu.SemaphoreType.DMA((2,)),
        pltpu.SemaphoreType.DMA((4,)),
    ]
    return call(back_kernel, pieces, weights, outs, scratch, 5)


def ahead_of(pieces, weights):
    rows = sum(p.shape[1] for p in pieces)
    depth, cols = weights.shape[0], weights.shape[1] // 2
    half = (rows // 2, depth)
    scratch = [
        pltpu.VMEM((rows, depth), BF16),
        pltpu.VMEM((depth, cols), BF16),
        pltpu.VMEM((depth, cols), BF16),
        pltpu.VMEM((rows, cols), BF16),
        pltpu.VMEM(half, BF16),
        pltpu.VMEM(half, BF16),
        pltpu.SemaphoreType.DMA((len(pieces),)),
        pltpu.SemaphoreType.DMA((2,)),
        pltpu.SemaphoreType.DMA((2,)),
    ]
    return call(ahead_kernel, pieces, weights, (half, half), scratch, 2)


def body(later_rows, earlier_rows, cotangent, up_weight, down_weight, up_total, down_total):
    n_dev = math.prod(lax.axis_size(a) for a in ALL)
    nz, nx = lax.axis_size("z"), lax.axis_size("x")
    factor = 1.0 / math.sqrt(later_rows.shape[0] * n_dev)
    weights = jnp.concatenate((up_weight, down_weight), axis=1)
    weights = gather(weights, "x").reshape(-1, weights.shape[1])
    weights = lax.all_gather(weights, "z", axis=0, tiled=True)
    pieces = gather_tokens((earlier_rows, cotangent, later_rows))
    down_term, up_term, mine, theirs = back(pieces, weights, nz, nx)
    down_term = lax.psum_scatter(down_term, "z", scatter_dimension=0, tiled=True)
    up_term = exchange_sum(up_term, "x").astype(BF16)
    up_term = exchange_sum(up_term, "z")
    earlier_grad = scatter_tokens(mine, theirs)
    mine, theirs = ahead_of(pieces, weights)
    later_out = scatter_tokens(mine, theirs)
    down_term = hop_sum(down_term.reshape(-1, *down_weight.shape), "x")
    up_updated = up_total + up_term * factor
    down_updated = down_total + down_term * factor
    return later_out, earlier_grad, up_updated, down_updated


def solution(mesh):
    n_tp = mesh.shape["tp"]
    finer = Mesh(mesh.devices.reshape(8, 4, n_tp // 2, 2), ALL)
    rows, weight = P(ALL, None), P(FS, ("y", "c"))
    return jax.shard_map(
        body,
        mesh=finer,
        in_specs=(rows, rows, rows, weight, weight, weight, weight),
        out_specs=(rows, rows, weight, weight),
        check_vma=False,
    )
```

```python
import math

import jax
import jax.numpy as jnp
from jax import lax
from jax.experimental import pallas as pl
from jax.experimental.pallas import tpu as pltpu
from jax.sharding import Mesh
from jax.sharding import PartitionSpec as P


FS = ("z", "x")
ALL = ("z", "x", "y", "c")
F32 = jnp.float32
BF16 = jnp.bfloat16
TILE = 512


def shift(x, axis, by):
    n = lax.axis_size(axis)
    return lax.ppermute(x, axis, [(i, (i + by) % n) for i in range(n)])


def gather_tokens(arrays):
    own = jnp.stack(arrays)
    half = own.shape[1] // 2
    behind, ahead = shift(own, "y", 1), shift(own, "y", -1)
    far_lo, far_hi = shift(behind[:, :half], "y", 1), shift(ahead[:, half:], "y", -1)
    pieces = (own, behind, ahead, far_lo, far_hi)
    partners = []
    for piece in pieces:
        partners.append(shift(piece, "c", 1))
    return (*pieces, *partners)


def plus(a, b):
    return (a.astype(F32) + b.astype(F32)).astype(BF16)


def scatter_tokens(mine, partners):
    partners = shift(partners, "c", 1)
    mine = plus(mine, partners)
    rows = mine.shape[0] // 4
    half = rows // 2
    own, behind, ahead, far = (mine[i * rows : (i + 1) * rows] for i in range(4))
    from_behind = shift(far[:half], "y", 1)
    from_ahead = shift(far[half:], "y", -1)
    ahead = jnp.concatenate([plus(ahead[:half], from_behind), ahead[half:]], axis=0)
    behind = jnp.concatenate([behind[:half], plus(behind[half:], from_ahead)], axis=0)
    a, b = shift(ahead, "y", 1), shift(behind, "y", -1)
    return (own.astype(F32) + a.astype(F32) + b.astype(F32)).astype(BF16)


def gather(x, axis):
    n = lax.axis_size(axis)
    return lax.all_to_all(jnp.broadcast_to(x[None], (n, *x.shape)), axis, 0, 0, tiled=True)


def exchange_sum(term, axis):
    tiles = lax.all_to_all(term, axis, 0, 0, tiled=True)
    return jnp.sum(tiles.astype(F32), axis=0)


def hop_sum(term, axis):
    n = lax.axis_size(axis)
    me = lax.axis_index(axis)

    def block(by):
        at = (me + by) & (n - 1)
        start = (at, *(0 for _ in term.shape[1:]))
        part = lax.dynamic_slice(term, start, (1, *term.shape[1:]), allow_negative_indices=False)
        return part[0]

    arrived = [shift(block(by), axis, by) for by in range(1, n)]
    return sum((a.astype(F32) for a in arrived), block(0).astype(F32))


def rows_times(left, right):
    return lax.dot_general(left, right, (((1,), (1,)), ((), ())), preferred_element_type=F32)


def over_tokens(left, right):
    return lax.dot_general(left, right, (((0,), (0,)), ((), ())), preferred_element_type=F32)


def copies(sources, target, sems, index):
    waits, row = [], 0
    for i, source in enumerate(sources):
        rows = source.shape[1]
        copy = pltpu.make_async_copy(source.at[index], target.at[pl.ds(row, rows)], sems.at[i])
        copy.start()
        waits.append((row, copy))
        row += rows
    return waits


def settle(waits, upto):
    while waits and waits[0][0] < upto:
        waits.pop(0)[1].wait()


def relu_times(rows, weight):
    return jnp.maximum(jnp.dot(rows, weight, preferred_element_type=F32), 0.0)


def up_kernel(*refs):
    pieces, (w, up_out, hid_out, pg_out) = refs[:10], refs[10:14]
    saved, cot, up, down, relu, hid, pg, ut, in_sems, w_sems, out_sems = refs[14:]
    cols = up.shape[1]
    up_copy = pltpu.make_async_copy(w.at[:, pl.ds(0, cols)], up, w_sems.at[0])
    up_copy.start()
    saved_waits = copies(pieces, saved, in_sems.at[0], 0)
    down_copy = pltpu.make_async_copy(w.at[:, pl.ds(cols, cols)], down, w_sems.at[1])
    down_copy.start()
    cot_waits = copies(pieces, cot, in_sems.at[1], 1)
    up_copy.wait()
    for t in range(0, saved.shape[0], TILE):
        settle(saved_waits, t + TILE)
        at = pl.ds(t, TILE)
        r = relu_times(saved[at], up[...])
        relu[at] = r
        hid[at] = (r * r).astype(BF16)
    down_copy.wait()
    for t in range(0, saved.shape[0], TILE):
        settle(cot_waits, t + TILE)
        at = pl.ds(t, TILE)
        grad = jnp.dot(cot[at], down[...], preferred_element_type=F32)
        pg[at] = (2.0 * relu[at] * grad).astype(BF16)
    hid_copy = pltpu.make_async_copy(hid, hid_out, out_sems.at[0])
    hid_copy.start()
    nx, nz, part = ut.shape[:3]

    @pl.loop(0, nz)
    def _(i):
        at = pl.ds(pl.multiple_of(i * nx * part, nx * part), nx * part)
        term = over_tokens(saved[:, at], pg[...]).astype(BF16)
        for j in range(nx):
            ut[j, i] = term[j * part : (j + 1) * part]

    pg_copy = pltpu.make_async_copy(pg, pg_out, out_sems.at[1])
    pg_copy.start()
    ut_copy = pltpu.make_async_copy(ut, up_out, out_sems.at[2])
    ut_copy.start()
    hid_copy.wait()
    pg_copy.wait()
    ut_copy.wait()


def down_kernel(*refs):
    pieces, (hid_in, down_out) = refs[:10], refs[10:12]
    cot, hid, dt, in_sems, sems = refs[12:]
    hid_copy = pltpu.make_async_copy(hid_in, hid, sems.at[0])
    hid_copy.start()
    settle(copies(pieces, cot, in_sems, 1), cot.shape[0])
    hid_copy.wait()
    block = dt.shape[0] // 8

    @pl.loop(0, 8)
    def _(i):
        at = pl.ds(pl.multiple_of(i * block, block), block)
        dt[at] = over_tokens(cot[:, at], hid[...]).astype(BF16)

    out_copy = pltpu.make_async_copy(dt, down_out, sems.at[1])
    out_copy.start()
    out_copy.wait()


def rows_kernel(pg_in, w, mine_out, theirs_out, pg, up, mine, theirs, sems):
    pg_copy = pltpu.make_async_copy(pg_in, pg, sems.at[0])
    up_copy = pltpu.make_async_copy(w.at[:, pl.ds(0, up.shape[1])], up, sems.at[1])
    pg_copy.start()
    up_copy.start()
    pg_copy.wait()
    up_copy.wait()
    first = pltpu.make_async_copy(mine, mine_out, sems.at[2])
    second = pltpu.make_async_copy(theirs, theirs_out, sems.at[3])
    outputs(pg, mine.shape[0], up, theirs)
    outputs(pg, 0, up, mine)
    second.start()
    first.start()
    first.wait()
    second.wait()


def outputs(hidden, first, weight, out):
    @pl.loop(0, out.shape[0], step=TILE)
    def _(t):
        rows = hidden[pl.ds(pl.multiple_of(first + t, TILE), TILE)]
        for n in range(0, out.shape[1], 512):
            part = rows_times(rows, weight[n : n + 512])
            out[pl.ds(pl.multiple_of(t, TILE), TILE), n : n + 512] = part.astype(BF16)


def ahead_kernel(*refs):
    pieces, (w, mine_out, theirs_out) = refs[:10], refs[10:13]
    rows, up, down, hid, mine, theirs, in_sems, w_sems, out_sems = refs[13:]
    cols = up.shape[1]
    up_copy = pltpu.make_async_copy(w.at[:, pl.ds(0, cols)], up, w_sems.at[0])
    up_copy.start()
    waits = copies(pieces, rows, in_sems, 2)
    down_copy = pltpu.make_async_copy(w.at[:, pl.ds(cols, cols)], down, w_sems.at[1])
    down_copy.start()
    up_copy.wait()
    for t in range(0, rows.shape[0], TILE):
        settle(waits, t + TILE)
        at = pl.ds(t, TILE)
        r = relu_times(rows[at], up[...])
        hid[at] = (r * r).astype(BF16)
    down_copy.wait()
    first = pltpu.make_async_copy(mine, mine_out, out_sems.at[0])
    second = pltpu.make_async_copy(theirs, theirs_out, out_sems.at[1])
    outputs(hid, mine.shape[0], down, theirs)
    outputs(hid, 0, down, mine)
    second.start()
    first.start()
    first.wait()
    second.wait()


def call(kernel, operands, outs, scratch, flops):
    hbm = pl.BlockSpec(memory_space=pltpu.HBM)
    return pl.pallas_call(
        kernel,
        out_shape=[jax.ShapeDtypeStruct(s, BF16) for s in outs],
        in_specs=[hbm] * len(operands),
        out_specs=[hbm] * len(outs),
        scratch_shapes=[pltpu.VMEM(*s) for s in scratch[0]]
        + [pltpu.SemaphoreType.DMA(s) for s in scratch[1]],
        cost_estimate=pl.CostEstimate(flops=flops, bytes_accessed=12 << 20, transcendentals=0),
        compiler_params=pltpu.CompilerParams(vmem_limit_bytes=60 * 1024 * 1024),
    )(*operands)


def products(pieces, weights, nz, nx):
    rows = sum(p.shape[1] for p in pieces)
    depth, cols = weights.shape[0], weights.shape[1] // 2
    n = len(pieces)
    flops = 2 * rows * depth * cols
    group, weight, wide = ((rows, depth), BF16), ((depth, cols), BF16), ((rows, cols), BF16)
    up_shape = (nx, nz, depth // (nx * nz), cols)
    half = (rows // 2, depth)

    def up_term():
        vmem = (group, group, weight, weight, (wide[0], F32), wide, wide, (up_shape, BF16))
        outs = (up_shape, wide[0], wide[0])
        return call(up_kernel, (*pieces, weights), outs, (vmem, ((2, n), (2,), (3,))), 3 * flops)

    def down_term(hidden):
        vmem = (group, wide, weight)
        return call(down_kernel, (*pieces, hidden), (weight[0],), (vmem, ((n,), (2,))), flops)[0]

    def row_grad(pre_grad):
        vmem = (wide, weight, (half, BF16), (half, BF16))
        return call(rows_kernel, (pre_grad, weights), (half, half), (vmem, ((4,),)), flops)

    def later():
        vmem = (group, weight, weight, wide, (half, BF16), (half, BF16))
        return call(
            ahead_kernel, (*pieces, weights), (half, half), (vmem, ((n,), (2,), (2,))), 2 * flops
        )

    return up_term, down_term, row_grad, later


def body(later_rows, earlier_rows, cotangent, up_weight, down_weight, up_total, down_total):
    n_dev = math.prod(lax.axis_size(a) for a in ALL)
    nz, nx = lax.axis_size("z"), lax.axis_size("x")
    factor = 1.0 / math.sqrt(later_rows.shape[0] * n_dev)
    weights = jnp.concatenate((up_weight, down_weight), axis=1)
    weights = gather(weights, "x").reshape(-1, weights.shape[1])
    weights = lax.all_gather(weights, "z", axis=0, tiled=True)
    pieces = gather_tokens((earlier_rows, cotangent, later_rows))
    grad_up, grad_down, grad_rows, ahead = products(pieces, weights, nz, nx)
    up_term, hidden, pre_grad = grad_up()
    up_term = exchange_sum(up_term, "x").astype(BF16)
    down_term = grad_down(hidden)
    down_term = lax.psum_scatter(down_term, "z", scatter_dimension=0, tiled=True)
    up_term = exchange_sum(up_term, "z")
    mine, theirs = grad_rows(pre_grad)
    earlier_grad = scatter_tokens(mine, theirs)
    mine, theirs = ahead()
    later_out = scatter_tokens(mine, theirs)
    down_term = hop_sum(down_term.reshape(-1, *down_weight.shape), "x")
    up_updated = up_total + up_term * factor
    down_updated = down_total + down_term * factor
    return later_out, earlier_grad, up_updated, down_updated


def solution(mesh):
    n_tp = mesh.shape["tp"]
    finer = Mesh(mesh.devices.reshape(8, 4, n_tp // 2, 2), ALL)
    rows, weight = P(ALL, None), P(FS, ("y", "c"))
    return jax.shard_map(
        body,
        mesh=finer,
        in_specs=(rows, rows, rows, weight, weight, weight, weight),
        out_specs=(rows, rows, weight, weight),
        check_vma=False,
    )
```

```python
import math

import jax
import jax.numpy as jnp
from jax import lax
from jax.experimental import pallas as pl
from jax.experimental.pallas import tpu as pltpu
from jax.sharding import Mesh
from jax.sharding import PartitionSpec as P


FS = ("z", "x")
ALL = ("z", "x", "y", "c")
F32 = jnp.float32
BF16 = jnp.bfloat16
TILE = 512


def shift(x, axis, by):
    n = lax.axis_size(axis)
    return lax.ppermute(x, axis, [(i, (i + by) % n) for i in range(n)])


def gather_tokens(arrays):
    own = jnp.stack(arrays)
    half = own.shape[1] // 2
    behind, ahead = shift(own, "y", 1), shift(own, "y", -1)
    far_lo, far_hi = shift(behind[:, :half], "y", 1), shift(ahead[:, half:], "y", -1)
    pieces = (own, behind, ahead, far_lo, far_hi)
    partners = []
    for piece in pieces:
        partners.append(shift(piece, "c", 1))
    return (*pieces, *partners)


def gather_later(own):
    behind, ahead, far = (shift(own, "y", by) for by in (1, -1, 2))
    mine = jnp.concatenate((own, behind, ahead, far), axis=0)[None]
    return mine, shift(mine, "c", 1)


def plus(a, b):
    return (a.astype(F32) + b.astype(F32)).astype(BF16)


def scatter_tokens(mine, partners):
    partners = shift(partners, "c", 1)
    rows = mine.shape[0] // 4
    at = [slice(i * rows, (i + 1) * rows) for i in range(4)]
    behind, ahead, far = (plus(mine[i], partners[i]) for i in at[1:])
    arrived = (shift(ahead, "y", 1), shift(behind, "y", -1), shift(far, "y", 2))
    total = mine[at[0]].astype(F32) + partners[at[0]].astype(F32)
    return sum((a.astype(F32) for a in arrived), total).astype(BF16)


def gather(x, axis):
    n = lax.axis_size(axis)
    return lax.all_to_all(jnp.broadcast_to(x[None], (n, *x.shape)), axis, 0, 0, tiled=True)


def exchange_sum(term, axis):
    tiles = lax.all_to_all(term, axis, 0, 0, tiled=True)
    return jnp.sum(tiles.astype(F32), axis=0)


def hop_sum(term, axis):
    n = lax.axis_size(axis)
    me = lax.axis_index(axis)

    def block(by):
        at = (me + by) & (n - 1)
        start = (at, *(0 for _ in term.shape[1:]))
        part = lax.dynamic_slice(term, start, (1, *term.shape[1:]), allow_negative_indices=False)
        return part[0]

    arrived = [shift(block(by), axis, by) for by in range(1, n)]
    return sum((a.astype(F32) for a in arrived), block(0).astype(F32))


def rows_times(left, right):
    return lax.dot_general(left, right, (((1,), (1,)), ((), ())), preferred_element_type=F32)


def over_tokens(left, right):
    return lax.dot_general(left, right, (((0,), (0,)), ((), ())), preferred_element_type=F32)


def copies(sources, target, sems, index):
    waits, row = [], 0
    for i, source in enumerate(sources):
        rows = source.shape[1]
        copy = pltpu.make_async_copy(source.at[index], target.at[pl.ds(row, rows)], sems.at[i])
        copy.start()
        waits.append((row, copy))
        row += rows
    return waits


def settle(waits, upto):
    while waits and waits[0][0] < upto:
        waits.pop(0)[1].wait()


def relu_times(rows, weight):
    return jnp.maximum(jnp.dot(rows, weight, preferred_element_type=F32), 0.0)


def pre_kernel(*refs):
    pieces, (w, down_out, relu_out) = refs[:10], refs[10:13]
    saved, cot, up, relu, hid, dt, in_sems, sems = refs[13:]
    up_copy = pltpu.make_async_copy(w, up, sems.at[0])
    up_copy.start()
    saved_waits = copies(pieces, saved, in_sems.at[0], 0)
    cot_waits = copies(pieces, cot, in_sems.at[1], 1)
    up_copy.wait()
    for t in range(0, saved.shape[0], TILE):
        settle(saved_waits, t + TILE)
        at = pl.ds(t, TILE)
        r = relu_times(saved[at], up[...])
        relu[at] = r
        hid[at] = (r * r).astype(BF16)
    settle(cot_waits, cot.shape[0])
    relu_copy = pltpu.make_async_copy(relu, relu_out, sems.at[1])
    block = dt.shape[0] // 8

    @pl.loop(0, 8)
    def _(i):
        at = pl.ds(pl.multiple_of(i * block, block), block)
        dt[at] = over_tokens(cot[:, at], hid[...]).astype(BF16)

    relu_copy.start()
    out_copy = pltpu.make_async_copy(dt, down_out, sems.at[2])
    out_copy.start()
    relu_copy.wait()
    out_copy.wait()


def place_down(parts, down, sems):
    n = len(parts)
    waits = []
    for k, part in enumerate(parts):
        at = (lax.axis_index("x") + (n - k)) & (n - 1)
        copy = pltpu.make_async_copy(part, down.at[:, at], sems.at[k])
        copy.start()
        waits.append(copy)
    return waits


def up_kernel(*refs):
    pieces, parts, (relu_in, up_out, pg_out) = refs[:10], refs[10:14], refs[14:17]
    saved, cot, down, relu, pg, ut, in_sems, w_sems, sems = refs[17:]
    down_waits = place_down(parts, down, w_sems)
    cot_waits = copies(pieces, cot, in_sems.at[1], 1)
    relu_copy = pltpu.make_async_copy(relu_in, relu, sems.at[0])
    relu_copy.start()
    saved_waits = copies(pieces, saved, in_sems.at[0], 0)
    for copy in down_waits:
        copy.wait()
    weight = down[...].reshape(-1, down.shape[-1])
    for t in range(0, cot.shape[0], TILE):
        settle(cot_waits, t + TILE)
        at = pl.ds(t, TILE)
        grad = jnp.dot(cot[at], weight, preferred_element_type=F32)
        if t == 0:
            relu_copy.wait()
        pg[at] = (2.0 * relu[at] * grad).astype(BF16)
    settle(saved_waits, saved.shape[0])
    nx, nz, part = ut.shape[:3]

    @pl.loop(0, nz)
    def _(i):
        at = pl.ds(pl.multiple_of(i * nx * part, nx * part), nx * part)
        term = over_tokens(saved[:, at], pg[...]).astype(BF16)
        for j in range(nx):
            ut[j, i] = term[j * part : (j + 1) * part]

    pg_copy = pltpu.make_async_copy(pg, pg_out, sems.at[1])
    pg_copy.start()
    ut_copy = pltpu.make_async_copy(ut, up_out, sems.at[2])
    ut_copy.start()
    pg_copy.wait()
    ut_copy.wait()


def rows_kernel(pg_in, w, mine_out, theirs_out, pg, up, mine, theirs, sems):
    pg_copy = pltpu.make_async_copy(pg_in, pg, sems.at[0])
    up_copy = pltpu.make_async_copy(w, up, sems.at[1])
    pg_copy.start()
    up_copy.start()
    pg_copy.wait()
    up_copy.wait()
    first = pltpu.make_async_copy(mine, mine_out, sems.at[2])
    second = pltpu.make_async_copy(theirs, theirs_out, sems.at[3])
    outputs(pg, mine.shape[0], up, theirs)
    outputs(pg, 0, up, mine)
    second.start()
    first.start()
    first.wait()
    second.wait()


def flat_rows(weight, first, count):
    each = weight.shape[1] * weight.shape[2]
    return weight[first // each : (first + count) // each].reshape(count, weight.shape[-1])


def outputs(hidden, first, weight, out):
    @pl.loop(0, out.shape[0], step=TILE)
    def _(t):
        rows = hidden[pl.ds(pl.multiple_of(first + t, TILE), TILE)]
        for n in range(0, out.shape[1], 512):
            block = weight[n : n + 512] if len(weight.shape) == 2 else flat_rows(weight, n, 512)
            part = rows_times(rows, block)
            out[pl.ds(pl.multiple_of(t, TILE), TILE), n : n + 512] = part.astype(BF16)


def ahead_kernel(*refs):
    pieces, parts, (w, mine_out, theirs_out) = refs[:2], refs[2:6], refs[6:9]
    rows, up, down, hid, mine, theirs, in_sems, w_sems, sems = refs[9:]
    up_copy = pltpu.make_async_copy(w, up, sems.at[0])
    up_copy.start()
    waits = copies(pieces, rows, in_sems, 0)
    down_waits = place_down(parts, down, w_sems)
    up_copy.wait()
    for t in range(0, rows.shape[0], TILE):
        settle(waits, t + TILE)
        at = pl.ds(t, TILE)
        r = relu_times(rows[at], up[...])
        hid[at] = (r * r).astype(BF16)
    for copy in down_waits:
        copy.wait()
    first = pltpu.make_async_copy(mine, mine_out, sems.at[1])
    second = pltpu.make_async_copy(theirs, theirs_out, sems.at[2])
    outputs(hid, mine.shape[0], down, theirs)
    outputs(hid, 0, down, mine)
    second.start()
    first.start()
    first.wait()
    second.wait()


def call(kernel, operands, outs, scratch, flops):
    hbm = pl.BlockSpec(memory_space=pltpu.HBM)
    return pl.pallas_call(
        kernel,
        out_shape=[jax.ShapeDtypeStruct(*s) for s in outs],
        in_specs=[hbm] * len(operands),
        out_specs=[hbm] * len(outs),
        scratch_shapes=[pltpu.VMEM(*s) for s in scratch[0]]
        + [pltpu.SemaphoreType.DMA(s) for s in scratch[1]],
        cost_estimate=pl.CostEstimate(flops=flops, bytes_accessed=12 << 20, transcendentals=0),
        compiler_params=pltpu.CompilerParams(vmem_limit_bytes=60 * 1024 * 1024),
    )(*operands)


def products(pieces, later, up, down, nz, nx):
    rows = sum(p.shape[1] for p in pieces)
    depth, cols = up.shape
    n = len(pieces)
    flops = 2 * rows * depth * cols
    group, weight, wide = ((rows, depth), BF16), ((depth, cols), BF16), ((rows, cols), BF16)
    relu = (wide[0], F32)
    part = depth // (nx * nz)
    split, up_shape = ((nz, nx, part, cols), BF16), ((nx, nz, part, cols), BF16)
    half = ((rows // 2, depth), BF16)

    def pre():
        scratch = (group, group, weight, relu, wide, weight), ((2, n), (3,))
        return call(pre_kernel, (*pieces, up), (weight, relu), scratch, 2 * flops)

    def up_term(relu_part):
        scratch = (group, group, split, relu, wide, up_shape), ((2, n), (nx,), (3,))
        operands = (*pieces, *down, relu_part)
        return call(up_kernel, operands, (up_shape, wide), scratch, 2 * flops)

    def row_grad(pre_grad):
        scratch = (wide, weight, half, half), ((4,),)
        return call(rows_kernel, (pre_grad, up), (half, half), scratch, flops)

    def ahead():
        scratch = (group, weight, split, wide, half, half), ((2,), (nx,), (3,))
        operands = (*later, *down, up)
        return call(ahead_kernel, operands, (half, half), scratch, 2 * flops)

    return pre, up_term, row_grad, ahead


def body(later_rows, earlier_rows, cotangent, up_weight, down_weight, up_total, down_total):
    n_dev = math.prod(lax.axis_size(a) for a in ALL)
    nz, nx = lax.axis_size("z"), lax.axis_size("x")
    factor = 1.0 / math.sqrt(later_rows.shape[0] * n_dev)
    up = gather(up_weight, "x").reshape(-1, up_weight.shape[1])
    up = lax.all_gather(up, "z", axis=0, tiled=True)
    down = gather(down_weight, "z")
    down = (down, *(shift(down, "x", by) for by in range(1, nx)))
    pieces = gather_tokens((earlier_rows, cotangent))
    later = gather_later(later_rows)
    pre, grad_up, grad_rows, ahead = products(pieces, later, up, down, nz, nx)
    down_term, relu = pre()
    down_term = lax.psum_scatter(down_term, "z", scatter_dimension=0, tiled=True)
    up_term, pre_grad = grad_up(relu)
    up_term = exchange_sum(up_term, "x").astype(BF16)
    up_term = exchange_sum(up_term, "z")
    mine, theirs = grad_rows(pre_grad)
    earlier_grad = scatter_tokens(mine, theirs)
    mine, theirs = ahead()
    later_out = scatter_tokens(mine, theirs)
    down_term = hop_sum(down_term.reshape(-1, *down_weight.shape), "x")
    up_updated = up_total + up_term * factor
    down_updated = down_total + down_term * factor
    return later_out, earlier_grad, up_updated, down_updated


def solution(mesh):
    n_tp = mesh.shape["tp"]
    finer = Mesh(mesh.devices.reshape(8, 4, n_tp // 2, 2), ALL)
    rows, weight = P(ALL, None), P(FS, ("y", "c"))
    return jax.shard_map(
        body,
        mesh=finer,
        in_specs=(rows, rows, rows, weight, weight, weight, weight),
        out_specs=(rows, rows, weight, weight),
        check_vma=False,
    )
```

```python
import math

import jax
import jax.numpy as jnp
from jax import lax
from jax.experimental import pallas as pl
from jax.experimental.pallas import tpu as pltpu
from jax.sharding import Mesh
from jax.sharding import PartitionSpec as P


FS = ("z", "x")
ALL = ("z", "x", "y", "c")
F32 = jnp.float32
BF16 = jnp.bfloat16
TILE = 512


def shift(x, axis, by):
    n = lax.axis_size(axis)
    return lax.ppermute(x, axis, [(i, (i + by) % n) for i in range(n)])


def gather_tokens(arrays):
    own = jnp.stack(arrays)
    half = own.shape[1] // 2
    behind, ahead = shift(own, "y", 1), shift(own, "y", -1)
    far_lo, far_hi = shift(behind[:, :half], "y", 1), shift(ahead[:, half:], "y", -1)
    pieces = (own, behind, ahead, far_lo, far_hi)
    partners = []
    for piece in pieces:
        partners.append(shift(piece, "c", 1))
    return (*pieces, *partners)


def gather_later(own):
    behind, ahead, far = (shift(own, "y", by) for by in (1, -1, 2))
    mine = jnp.concatenate((own, behind, ahead, far), axis=0)[None]
    return mine, shift(mine, "c", 1)


def plus(a, b):
    return (a.astype(F32) + b.astype(F32)).astype(BF16)


def scatter_tokens(mine, partners):
    partners = shift(partners, "c", 1)
    rows = mine.shape[0] // 4
    at = [slice(i * rows, (i + 1) * rows) for i in range(4)]
    behind, ahead, far = (plus(mine[i], partners[i]) for i in at[1:])
    arrived = (shift(ahead, "y", 1), shift(behind, "y", -1), shift(far, "y", 2))
    total = mine[at[0]].astype(F32) + partners[at[0]].astype(F32)
    return sum((a.astype(F32) for a in arrived), total).astype(BF16)


def gather(x, axis):
    n = lax.axis_size(axis)
    return lax.all_to_all(jnp.broadcast_to(x[None], (n, *x.shape)), axis, 0, 0, tiled=True)


def exchange_sum(term, axis):
    tiles = lax.all_to_all(term, axis, 0, 0, tiled=True)
    return jnp.sum(tiles.astype(F32), axis=0)


def hop_sum(term, axis):
    n = lax.axis_size(axis)
    me = lax.axis_index(axis)

    def block(by):
        at = (me + by) & (n - 1)
        start = (at, *(0 for _ in term.shape[1:]))
        part = lax.dynamic_slice(term, start, (1, *term.shape[1:]), allow_negative_indices=False)
        return part[0]

    arrived = [shift(block(by), axis, by) for by in range(1, n)]
    return sum((a.astype(F32) for a in arrived), block(0).astype(F32))


def rows_times(left, right):
    return lax.dot_general(left, right, (((1,), (1,)), ((), ())), preferred_element_type=F32)


def over_tokens(left, right):
    return lax.dot_general(left, right, (((0,), (0,)), ((), ())), preferred_element_type=F32)


def copies(sources, target, sems, index):
    waits, row = [], 0
    for i, source in enumerate(sources):
        rows = source.shape[1]
        copy = pltpu.make_async_copy(source.at[index], target.at[pl.ds(row, rows)], sems.at[i])
        copy.start()
        waits.append((row, copy))
        row += rows
    return waits


def settle(waits, upto):
    while waits and waits[0][0] < upto:
        waits.pop(0)[1].wait()


def relu_times(rows, weight):
    return jnp.maximum(jnp.dot(rows, weight, preferred_element_type=F32), 0.0)


def pre_kernel(*refs):
    pieces, (w, down_out, relu_out) = refs[:10], refs[10:13]
    saved, cot, up, relu, hid, dt, in_sems, sems = refs[13:]
    up_copy = pltpu.make_async_copy(w, up, sems.at[0])
    up_copy.start()
    saved_waits = copies(pieces, saved, in_sems.at[0], 0)
    cot_waits = copies(pieces, cot, in_sems.at[1], 1)
    up_copy.wait()
    for t in range(0, saved.shape[0], TILE):
        settle(saved_waits, t + TILE)
        at = pl.ds(t, TILE)
        r = relu_times(saved[at], up[...])
        relu[at] = r
        hid[at] = (r * r).astype(BF16)
    settle(cot_waits, cot.shape[0])
    nx, nz, part = dt.shape[:3]

    def terms(first, last):
        @pl.loop(first, last)
        def _(i):
            at = pl.ds(pl.multiple_of(i * nx * part, nx * part), nx * part)
            term = over_tokens(cot[:, at], hid[...]).astype(BF16)
            for j in range(nx):
                dt[j, i] = term[j * part : (j + 1) * part]

        piece = pl.ds(first, last - first)
        return pltpu.make_async_copy(dt.at[:, piece], down_out.at[:, piece], sems.at[first and 3 or 2])

    early = terms(0, nz * 3 // 4)
    relu_copy = pltpu.make_async_copy(relu, relu_out, sems.at[1])
    relu_copy.start()
    early.start()
    late = terms(nz * 3 // 4, nz)
    late.start()
    relu_copy.wait()
    early.wait()
    late.wait()


def place_down(parts, down, sems):
    n = len(parts)
    waits = []
    for k, part in enumerate(parts):
        at = (lax.axis_index("x") + (n - k)) & (n - 1)
        copy = pltpu.make_async_copy(part, down.at[:, at], sems.at[k])
        copy.start()
        waits.append(copy)
    return waits


def grad_kernel(*refs):
    pieces, parts, (relu_in, w, pg_out, mine_out, theirs_out) = refs[:10], refs[10:14], refs[14:19]
    cot, down, up, relu, pg, mine, theirs, in_sems, w_sems, sems = refs[19:]
    down_waits = place_down(parts, down, w_sems)
    cot_waits = copies(pieces, cot, in_sems, 1)
    relu_copy = pltpu.make_async_copy(relu_in, relu, sems.at[0])
    relu_copy.start()
    up_copy = pltpu.make_async_copy(w, up, sems.at[1])
    up_copy.start()
    for copy in down_waits:
        copy.wait()
    weight = down[...].reshape(-1, down.shape[-1])
    for t in range(0, cot.shape[0], TILE):
        settle(cot_waits, t + TILE)
        at = pl.ds(t, TILE)
        grad = jnp.dot(cot[at], weight, preferred_element_type=F32)
        if t == 0:
            relu_copy.wait()
        pg[at] = (2.0 * relu[at] * grad).astype(BF16)
    up_copy.wait()
    pg_copy = pltpu.make_async_copy(pg, pg_out, sems.at[2])
    first = pltpu.make_async_copy(mine, mine_out, sems.at[3])
    second = pltpu.make_async_copy(theirs, theirs_out, sems.at[4])
    outputs(pg, mine.shape[0], up, theirs, pg_copy)
    outputs(pg, 0, up, mine, second)
    first.start()
    for copy in (pg_copy, second, first):
        copy.wait()


def up_kernel(*refs):
    pieces, (pg_in, up_out) = refs[:10], refs[10:12]
    saved, pg, ut, in_sems, sems = refs[12:]
    pg_copy = pltpu.make_async_copy(pg_in, pg, sems.at[0])
    pg_copy.start()
    waits = copies(pieces, saved, in_sems, 0)
    pg_copy.wait()
    settle(waits, saved.shape[0])
    block = 256
    depth = ut.shape[0]

    def terms(first, last):
        @pl.loop(first, last, step=block)
        def _(i):
            at = pl.ds(pl.multiple_of(i, block), block)
            ut[at] = over_tokens(saved[:, at], pg[...]).astype(BF16)

        piece = pl.ds(first, last - first)
        return pltpu.make_async_copy(ut.at[piece], up_out.at[piece], sems.at[first and 2 or 1])

    early = terms(0, depth * 3 // 4)
    early.start()
    late = terms(depth * 3 // 4, depth)
    late.start()
    early.wait()
    late.wait()


def flat_rows(weight, first, count):
    each = weight.shape[1] * weight.shape[2]
    return weight[first // each : (first + count) // each].reshape(count, weight.shape[-1])


def outputs(hidden, first, weight, out, copy=None):
    rows = hidden[pl.ds(first, out.shape[0])]
    for n in range(0, out.shape[1], 512):
        block = weight[n : n + 512] if len(weight.shape) == 2 else flat_rows(weight, n, 512)
        out[:, n : n + 512] = rows_times(rows, block).astype(BF16)
        if copy is not None and n == 512:
            copy.start()


def ahead_kernel(*refs):
    pieces, parts, (w, mine_out, theirs_out) = refs[:2], refs[2:6], refs[6:9]
    rows, up, down, hid, mine, theirs, in_sems, w_sems, sems = refs[9:]
    up_copy = pltpu.make_async_copy(w, up, sems.at[0])
    up_copy.start()
    waits = copies(pieces, rows, in_sems, 0)
    down_waits = place_down(parts, down, w_sems)
    up_copy.wait()
    for t in range(0, rows.shape[0], TILE):
        settle(waits, t + TILE)
        at = pl.ds(t, TILE)
        r = relu_times(rows[at], up[...])
        hid[at] = (r * r).astype(BF16)
    for copy in down_waits:
        copy.wait()
    first = pltpu.make_async_copy(mine, mine_out, sems.at[1])
    second = pltpu.make_async_copy(theirs, theirs_out, sems.at[2])
    outputs(hid, mine.shape[0], down, theirs)
    outputs(hid, 0, down, mine, second)
    first.start()
    first.wait()
    second.wait()


def call(kernel, operands, outs, scratch, flops):
    hbm = pl.BlockSpec(memory_space=pltpu.HBM)
    return pl.pallas_call(
        kernel,
        out_shape=[jax.ShapeDtypeStruct(*s) for s in outs],
        in_specs=[hbm] * len(operands),
        out_specs=[hbm] * len(outs),
        scratch_shapes=[pltpu.VMEM(*s) for s in scratch[0]]
        + [pltpu.SemaphoreType.DMA(s) for s in scratch[1]],
        cost_estimate=pl.CostEstimate(flops=flops, bytes_accessed=12 << 20, transcendentals=0),
        compiler_params=pltpu.CompilerParams(vmem_limit_bytes=60 * 1024 * 1024),
    )(*operands)


def products(pieces, later, up, down, nz, nx):
    rows = sum(p.shape[1] for p in pieces)
    depth, cols = up.shape
    n = len(pieces)
    flops = 2 * rows * depth * cols
    group, weight, wide = ((rows, depth), BF16), ((depth, cols), BF16), ((rows, cols), BF16)
    relu = (wide[0], F32)
    part = depth // (nx * nz)
    split, swapped = ((nz, nx, part, cols), BF16), ((nx, nz, part, cols), BF16)
    half = ((rows // 2, depth), BF16)

    def pre():
        scratch = (group, group, weight, relu, wide, swapped), ((2, n), (4,))
        return call(pre_kernel, (*pieces, up), (swapped, relu), scratch, 2 * flops)

    def grad(relu_part):
        scratch = (group, split, weight, relu, wide, half, half), ((n,), (nx,), (5,))
        operands = (*pieces, *down, relu_part, up)
        return call(grad_kernel, operands, (wide, half, half), scratch, 2 * flops)

    def up_term(pre_grad):
        scratch = (group, wide, weight), ((n,), (3,))
        return call(up_kernel, (*pieces, pre_grad), (weight,), scratch, flops)[0]

    def ahead():
        scratch = (group, weight, split, wide, half, half), ((2,), (nx,), (3,))
        operands = (*later, *down, up)
        return call(ahead_kernel, operands, (half, half), scratch, 2 * flops)

    return pre, grad, up_term, ahead


def body(later_rows, earlier_rows, cotangent, up_weight, down_weight, up_total, down_total):
    n_dev = math.prod(lax.axis_size(a) for a in ALL)
    nz, nx = lax.axis_size("z"), lax.axis_size("x")
    factor = 1.0 / math.sqrt(later_rows.shape[0] * n_dev)
    up = gather(up_weight, "x").reshape(-1, up_weight.shape[1])
    up = lax.all_gather(up, "z", axis=0, tiled=True)
    down = gather(down_weight, "z")
    down = (down, *(shift(down, "x", by) for by in range(1, nx)))
    pieces = gather_tokens((earlier_rows, cotangent))
    later = gather_later(later_rows)
    pre, grad, grad_up, ahead = products(pieces, later, up, down, nz, nx)
    down_term, relu = pre()
    down_term = exchange_sum(down_term, "x").astype(BF16)
    pre_grad, mine, theirs = grad(relu)
    earlier_grad = scatter_tokens(mine, theirs)
    up_term = grad_up(pre_grad)
    up_term = lax.psum_scatter(up_term, "z", scatter_dimension=0, tiled=True)
    down_term = exchange_sum(down_term, "z")
    mine, theirs = ahead()
    later_out = scatter_tokens(mine, theirs)
    up_term = hop_sum(up_term.reshape(-1, *up_weight.shape), "x")
    up_updated = up_total + up_term * factor
    down_updated = down_total + down_term * factor
    return later_out, earlier_grad, up_updated, down_updated


def solution(mesh):
    n_tp = mesh.shape["tp"]
    finer = Mesh(mesh.devices.reshape(8, 4, n_tp // 2, 2), ALL)
    rows, weight = P(ALL, None), P(FS, ("y", "c"))
    return jax.shard_map(
        body,
        mesh=finer,
        in_specs=(rows, rows, rows, weight, weight, weight, weight),
        out_specs=(rows, rows, weight, weight),
        check_vma=False,
    )
```

```python
import math

import jax
import jax.numpy as jnp
from jax import lax
from jax.experimental import pallas as pl
from jax.experimental.pallas import tpu as pltpu
from jax.sharding import Mesh
from jax.sharding import PartitionSpec as P


FS = ("z", "x")
ALL = ("z", "x", "y", "c")
F32 = jnp.float32
BF16 = jnp.bfloat16
TILE = 512


def shift(x, axis, by):
    n = lax.axis_size(axis)
    return lax.ppermute(x, axis, [(i, (i + by) % n) for i in range(n)])


def gather_tokens(arrays):
    own = jnp.stack(arrays)
    half = own.shape[1] // 2
    behind, ahead = shift(own, "y", 1), shift(own, "y", -1)
    far_lo, far_hi = shift(behind[:, :half], "y", 1), shift(ahead[:, half:], "y", -1)
    pieces = (own, behind, ahead, far_lo, far_hi)
    partners = []
    for piece in pieces:
        partners.append(shift(piece, "c", 1))
    return (*pieces, *partners)


def gather_later(own):
    behind, ahead, far = (shift(own, "y", by) for by in (1, -1, 2))
    mine = jnp.concatenate((own, behind, ahead, far), axis=0)[None]
    return mine, shift(mine, "c", 1)


def plus(a, b):
    return (a.astype(F32) + b.astype(F32)).astype(BF16)


def scatter_tokens(mine, partners):
    partners = shift(partners, "c", 1)
    rows = mine.shape[0] // 4
    at = [slice(i * rows, (i + 1) * rows) for i in range(4)]
    behind, ahead, far = (plus(mine[i], partners[i]) for i in at[1:])
    arrived = (shift(ahead, "y", 1), shift(behind, "y", -1), shift(far, "y", 2))
    total = mine[at[0]].astype(F32) + partners[at[0]].astype(F32)
    return sum((a.astype(F32) for a in arrived), total).astype(BF16)


def gather(x, axis):
    n = lax.axis_size(axis)
    return lax.all_to_all(jnp.broadcast_to(x[None], (n, *x.shape)), axis, 0, 0, tiled=True)


def exchange_sum(term, axis):
    tiles = lax.all_to_all(term, axis, 0, 0, tiled=True)
    return jnp.sum(tiles.astype(F32), axis=0)


def hop_sum(term, axis):
    n = lax.axis_size(axis)
    me = lax.axis_index(axis)

    def block(by):
        at = (me + by) & (n - 1)
        start = (at, *(0 for _ in term.shape[1:]))
        part = lax.dynamic_slice(term, start, (1, *term.shape[1:]), allow_negative_indices=False)
        return part[0]

    arrived = [shift(block(by), axis, by) for by in range(1, n)]
    return sum((a.astype(F32) for a in arrived), block(0).astype(F32))


def rows_times(left, right):
    return lax.dot_general(left, right, (((1,), (1,)), ((), ())), preferred_element_type=F32)


def over_tokens(left, right):
    return lax.dot_general(left, right, (((0,), (0,)), ((), ())), preferred_element_type=F32)


def copies(sources, target, sems, index):
    waits, row = [], 0
    for i, source in enumerate(sources):
        rows = source.shape[1]
        copy = pltpu.make_async_copy(source.at[index], target.at[pl.ds(row, rows)], sems.at[i])
        copy.start()
        waits.append((row, copy))
        row += rows
    return waits


def settle(waits, upto):
    while waits and waits[0][0] < upto:
        waits.pop(0)[1].wait()


def relu_times(rows, weight):
    return jnp.maximum(jnp.dot(rows, weight, preferred_element_type=F32), 0.0)


def place_weights(first, parts, target, col, width, sems):
    n = len(parts)
    pairs = [(first.at[:, :, :, pl.ds(col, width)], target.at[:, :, :, pl.ds(0, width)])]
    for k, part in enumerate(parts):
        at = (lax.axis_index("x") + (n - k)) & (n - 1)
        pairs.append((part.at[:, :, pl.ds(col, width)], target.at[:, at, :, pl.ds(width, width)]))
    waits = [pltpu.make_async_copy(a, b, sems.at[i]) for i, (a, b) in enumerate(pairs)]
    for copy in waits:
        copy.start()
    return waits


def half_products(pieces, weight_copies, saved, cot, weight, hid, pg, pg_out, store, flush, in_sems, sem):
    for copy in weight_copies:
        copy.start()
    saved_waits = copies(pieces, saved, in_sems.at[0], 0)
    cot_waits = copies(pieces, cot, in_sems.at[1], 1)
    for copy in weight_copies:
        copy.wait()
    width = hid.shape[1]
    both = weight[...].reshape(-1, 2 * width)
    for t in range(0, saved.shape[0], TILE):
        at = pl.ds(t, TILE)
        settle(saved_waits, t + TILE)
        r = relu_times(saved[at], both[:, :width])
        hid[at] = (r * r).astype(BF16)
        settle(cot_waits, t + TILE)
        grad = jnp.dot(cot[at], both[:, width:], preferred_element_type=F32)
        pg[at] = (2.0 * r * grad).astype(BF16)
    nz, block = weight.shape[0], weight.shape[1] * weight.shape[2]

    def terms(first, last):
        @pl.loop(first, last)
        def _(i):
            at = pl.ds(pl.multiple_of(i * block, block), block)
            store(i, 0, over_tokens(saved[:, at], pg[...]).astype(BF16))
            store(i, width, over_tokens(cot[:, at], hid[...]).astype(BF16))

        return flush(first, last)

    early = terms(0, nz * 3 // 4)
    pg_copy = pltpu.make_async_copy(pg, pg_out, sem)
    pg_copy.start()
    early.start()
    late = terms(nz * 3 // 4, nz)
    late.start()
    for copy in (pg_copy, early, late):
        copy.wait()


def first_kernel(*refs):
    pieces, (w, out, pg_out) = refs[:10], refs[10:13]
    saved, cot, weight, hid, pg, term, in_sems, sems = refs[13:]
    block = weight.shape[1] * weight.shape[2]

    def store(i, col, value):
        rows = pl.ds(pl.multiple_of(i * block, block), block)
        term[rows, col : col + value.shape[1]] = value

    def flush(first, last):
        rows = pl.ds(first * block, (last - first) * block)
        return pltpu.make_async_copy(term.at[rows], out.at[rows], sems.at[2 if first else 1])

    weight_copies = [pltpu.make_async_copy(w, weight, sems.at[0])]
    half_products(
        pieces, weight_copies, saved, cot, weight, hid, pg, pg_out, store, flush, in_sems, sems.at[3]
    )


def second_kernel(*refs):
    pieces, parts, (out, pg_out) = refs[:10], refs[10:14], refs[14:16]
    saved, cot, weight, hid, pg, term, in_sems, w_sems, sems = refs[16:]
    nx, _, part = term.shape[:3]

    def store(i, col, value):
        for j in range(nx):
            term[j, i, :, col : col + value.shape[1]] = value[j * part : (j + 1) * part]

    def flush(first, last):
        at = pl.ds(first, last - first)
        return pltpu.make_async_copy(term.at[:, at], out.at[:, at], sems.at[2 if first else 1])

    weight_copies = []
    for k, piece in enumerate(parts):
        at = (lax.axis_index("x") + (nx - k)) & (nx - 1)
        weight_copies.append(pltpu.make_async_copy(piece, weight.at[:, at], w_sems.at[k]))
    half_products(
        pieces, weight_copies, saved, cot, weight, hid, pg, pg_out, store, flush, in_sems, sems.at[3]
    )


def rows_kernel(*refs):
    (pg_a, pg_b, first), parts, (mine_out, theirs_out) = refs[:3], refs[3:7], refs[7:9]
    pg, up, mine, theirs, w_sems, sems = refs[9:]
    width = pg.shape[1] // 2
    a = pltpu.make_async_copy(pg_a, pg.at[:, pl.ds(0, width)], sems.at[0])
    b = pltpu.make_async_copy(pg_b, pg.at[:, pl.ds(width, width)], sems.at[1])
    a.start()
    b.start()
    waits = place_weights(first, parts, up, 0, width, w_sems)
    for copy in (a, b, *waits):
        copy.wait()
    mine_copy = pltpu.make_async_copy(mine, mine_out, sems.at[2])
    theirs_copy = pltpu.make_async_copy(theirs, theirs_out, sems.at[3])
    outputs(pg, mine.shape[0], up, theirs)
    outputs(pg, 0, up, mine, theirs_copy)
    mine_copy.start()
    theirs_copy.wait()
    mine_copy.wait()


def flat_rows(weight, first, count):
    each = weight.shape[1] * weight.shape[2]
    return weight[first // each : (first + count) // each].reshape(count, weight.shape[-1])


def outputs(hidden, first, weight, out, copy=None):
    rows = hidden[pl.ds(first, out.shape[0])]
    for n in range(0, out.shape[1], 512):
        out[:, n : n + 512] = rows_times(rows, flat_rows(weight, n, 512)).astype(BF16)
        if copy is not None and n == 512:
            copy.start()


def ahead_kernel(*refs):
    pieces, first, parts, (mine_out, theirs_out) = refs[:2], refs[2], refs[3:7], refs[7:9]
    rows, up, down, hid, mine, theirs, in_sems, w_sems, sems = refs[9:]
    width = hid.shape[1] // 2
    up_waits = place_weights(first, parts, up, 0, width, w_sems.at[0])
    waits = copies(pieces, rows, in_sems, 0)
    down_waits = place_weights(first, parts, down, width, width, w_sems.at[1])
    for copy in up_waits:
        copy.wait()
    weight = up[...].reshape(-1, 2 * width)
    for t in range(0, rows.shape[0], TILE):
        settle(waits, t + TILE)
        at = pl.ds(t, TILE)
        r = relu_times(rows[at], weight)
        hid[at] = (r * r).astype(BF16)
    for copy in down_waits:
        copy.wait()
    mine_copy = pltpu.make_async_copy(mine, mine_out, sems.at[0])
    theirs_copy = pltpu.make_async_copy(theirs, theirs_out, sems.at[1])
    outputs(hid, mine.shape[0], down, theirs)
    outputs(hid, 0, down, mine, theirs_copy)
    mine_copy.start()
    theirs_copy.wait()
    mine_copy.wait()


def call(kernel, operands, outs, scratch, flops):
    hbm = pl.BlockSpec(memory_space=pltpu.HBM)
    return pl.pallas_call(
        kernel,
        out_shape=[jax.ShapeDtypeStruct(*s) for s in outs],
        in_specs=[hbm] * len(operands),
        out_specs=[hbm] * len(outs),
        scratch_shapes=[pltpu.VMEM(*s) for s in scratch[0]]
        + [pltpu.SemaphoreType.DMA(s) for s in scratch[1]],
        cost_estimate=pl.CostEstimate(flops=flops, bytes_accessed=12 << 20, transcendentals=0),
        compiler_params=pltpu.CompilerParams(vmem_limit_bytes=60 * 1024 * 1024),
    )(*operands)


def products(pieces, later, first, parts):
    rows = sum(p.shape[1] for p in pieces)
    nz, nx, part, cols = first.shape
    depth, width = nz * nx * part, cols // 2
    n = len(pieces)
    flops = 2 * rows * depth * cols
    group, wide = ((rows, depth), BF16), ((rows, cols), BF16)
    split, swapped, flat = (
        ((nz, nx, part, cols), BF16),
        ((nx, nz, part, cols), BF16),
        ((depth, cols), BF16),
    )
    narrow, half = ((rows, width), BF16), ((rows // 2, depth), BF16)

    def one():
        scratch = (group, group, split, narrow, narrow, flat), ((2, n), (4,))
        return call(first_kernel, (*pieces, first), (flat, narrow), scratch, 2 * flops)

    def two():
        scratch = (group, group, split, narrow, narrow, swapped), ((2, n), (nx,), (4,))
        return call(second_kernel, (*pieces, *parts), (swapped, narrow), scratch, 2 * flops)

    def row_grad(pg_a, pg_b):
        scratch = (wide, split, half, half), ((nx + 1,), (4,))
        return call(rows_kernel, (pg_a, pg_b, first, *parts), (half, half), scratch, flops)

    def ahead():
        scratch = (group, split, split, wide, half, half), ((2,), (2, nx + 1), (2,))
        return call(ahead_kernel, (*later, first, *parts), (half, half), scratch, 2 * flops)

    return one, two, row_grad, ahead


def body(later_rows, earlier_rows, cotangent, up_weight, down_weight, up_total, down_total):
    n_dev = math.prod(lax.axis_size(a) for a in ALL)
    nz, nx = lax.axis_size("z"), lax.axis_size("x")
    factor = 1.0 / math.sqrt(later_rows.shape[0] * n_dev)
    width = up_weight.shape[1] // 2
    low = jnp.concatenate((up_weight[:, :width], down_weight[:, :width]), axis=1)
    high = jnp.concatenate((up_weight[:, width:], down_weight[:, width:]), axis=1)
    low = gather(low, "x").reshape(-1, low.shape[1])
    low = lax.all_gather(low, "z", axis=0, tiled=True).reshape(nz, nx, *high.shape)
    high = gather(high, "z")
    high = (high, *(shift(high, "x", by) for by in range(1, nx)))
    pieces = gather_tokens((earlier_rows, cotangent))
    later = gather_later(later_rows)
    one, two, row_grad, ahead = products(pieces, later, low, high)
    low_terms, low_pg = one()
    low_terms = lax.psum_scatter(low_terms, "z", scatter_dimension=0, tiled=True)
    high_terms, high_pg = two()
    high_terms = exchange_sum(high_terms, "x").astype(BF16)
    mine, theirs = row_grad(low_pg, high_pg)
    earlier_grad = scatter_tokens(mine, theirs)
    high_terms = exchange_sum(high_terms, "z")
    mine, theirs = ahead()
    later_out = scatter_tokens(mine, theirs)
    low_terms = hop_sum(low_terms.reshape(-1, *up_weight.shape), "x")
    up_term = jnp.concatenate((low_terms[:, :width], high_terms[:, :width]), axis=1)
    down_term = jnp.concatenate((low_terms[:, width:], high_terms[:, width:]), axis=1)
    up_updated = up_total + up_term * factor
    down_updated = down_total + down_term * factor
    return later_out, earlier_grad, up_updated, down_updated


def solution(mesh):
    n_tp = mesh.shape["tp"]
    finer = Mesh(mesh.devices.reshape(8, 4, n_tp // 2, 2), ALL)
    rows, weight = P(ALL, None), P(FS, ("y", "c"))
    return jax.shard_map(
        body,
        mesh=finer,
        in_specs=(rows, rows, rows, weight, weight, weight, weight),
        out_specs=(rows, rows, weight, weight),
        check_vma=False,
    )
```

```python
import math

import jax
import jax.numpy as jnp
from jax import lax
from jax.experimental import pallas as pl
from jax.experimental.pallas import tpu as pltpu
from jax.sharding import Mesh
from jax.sharding import PartitionSpec as P


FS = ("z", "x")
ALL = ("z", "x", "y", "c")
F32 = jnp.float32
BF16 = jnp.bfloat16
TILE = 512


def shift(x, axis, by):
    n = lax.axis_size(axis)
    return lax.ppermute(x, axis, [(i, (i + by) % n) for i in range(n)])


def gather_tokens(arrays):
    own = jnp.stack(arrays)
    half = own.shape[1] // 2
    behind, ahead = shift(own, "y", 1), shift(own, "y", -1)
    far_lo, far_hi = shift(behind[:, :half], "y", 1), shift(ahead[:, half:], "y", -1)
    pieces = (own, behind, ahead, far_lo, far_hi)
    partners = []
    for piece in pieces:
        partners.append(shift(piece, "c", 1))
    return (*pieces, *partners)


def gather_later(own):
    behind, ahead, far = (shift(own, "y", by) for by in (1, -1, 2))
    mine = jnp.concatenate((own, behind, ahead, far), axis=0)[None]
    return mine, shift(mine, "c", 1)


def plus(a, b):
    return (a.astype(F32) + b.astype(F32)).astype(BF16)


def scatter_tokens(mine, partners):
    partners = shift(partners, "c", 1)
    rows = mine.shape[0] // 4
    at = [slice(i * rows, (i + 1) * rows) for i in range(4)]
    behind, ahead, far = (plus(mine[i], partners[i]) for i in at[1:])
    arrived = (shift(ahead, "y", 1), shift(behind, "y", -1), shift(far, "y", 2))
    total = mine[at[0]].astype(F32) + partners[at[0]].astype(F32)
    return sum((a.astype(F32) for a in arrived), total).astype(BF16)


def gather(x, axis):
    n = lax.axis_size(axis)
    return lax.all_to_all(jnp.broadcast_to(x[None], (n, *x.shape)), axis, 0, 0, tiled=True)


def exchange_sum(term, axis):
    tiles = lax.all_to_all(term, axis, 0, 0, tiled=True)
    return jnp.sum(tiles.astype(F32), axis=0)


def hop_sum(term, axis):
    n = lax.axis_size(axis)
    me = lax.axis_index(axis)

    def block(by):
        at = (me + by) & (n - 1)
        start = (at, *(0 for _ in term.shape[1:]))
        part = lax.dynamic_slice(term, start, (1, *term.shape[1:]), allow_negative_indices=False)
        return part[0]

    arrived = [shift(block(by), axis, by) for by in range(1, n)]
    return sum((a.astype(F32) for a in arrived), block(0).astype(F32))


def rows_times(left, right):
    return lax.dot_general(left, right, (((1,), (1,)), ((), ())), preferred_element_type=F32)


def copies(sources, target, sems, index):
    waits, row = [], 0
    for i, source in enumerate(sources):
        rows = source.shape[1]
        copy = pltpu.make_async_copy(source.at[index], target.at[pl.ds(row, rows)], sems.at[i])
        copy.start()
        waits.append((row, copy))
        row += rows
    return waits


def settle(waits, upto):
    while waits and waits[0][0] < upto:
        waits.pop(0)[1].wait()


def relu_times(rows, weight):
    return jnp.maximum(jnp.dot(rows, weight, preferred_element_type=F32), 0.0)


def place_weights(first, parts, target, col, width, sems):
    n = len(parts)
    pairs = [(first.at[:, :, :, pl.ds(col, width)], target.at[:, :, :, pl.ds(0, width)])]
    for k, part in enumerate(parts):
        at = (lax.axis_index("x") + (n - k)) & (n - 1)
        pairs.append((part.at[:, :, pl.ds(col, width)], target.at[:, at, :, pl.ds(width, width)]))
    waits = [pltpu.make_async_copy(a, b, sems.at[i]) for i, (a, b) in enumerate(pairs)]
    for copy in waits:
        copy.start()
    return waits


def half_products(pieces, weight_copies, saved, cot, weight, hid, pg_t, pg, pg_out, store, flush, in_sems, sem):
    for copy in weight_copies:
        copy.start()
    saved_waits = copies(pieces, saved, in_sems.at[0], 0)
    for copy in weight_copies:
        copy.wait()
    cot_waits = copies(pieces, cot, in_sems.at[1], 1)
    width = hid.shape[0]
    both = weight[...].reshape(-1, 2 * width)
    for t in range(0, saved.shape[0], TILE):
        at = pl.ds(t, TILE)
        settle(saved_waits, t + TILE)
        r = relu_times(saved[at], both[:, :width])
        hid[:, at] = (r * r).astype(BF16).T
        settle(cot_waits, t + TILE)
        grad = jnp.dot(cot[at], both[:, width:], preferred_element_type=F32)
        piece = (2.0 * r * grad).astype(BF16)
        pg[at] = piece
        pg_t[:, at] = piece.T
    nz, block = weight.shape[0], weight.shape[1] * weight.shape[2]

    def terms(first, last):
        @pl.loop(first, last, step=2)
        def _(i):
            at = pl.ds(pl.multiple_of(i * block, 2 * block), 2 * block)
            up = jnp.dot(pg_t[...], saved[:, at], preferred_element_type=F32).astype(BF16).T
            down = jnp.dot(hid[...], cot[:, at], preferred_element_type=F32).astype(BF16).T
            for j in range(2):
                store(i + j, 0, up[j * block : (j + 1) * block])
                store(i + j, width, down[j * block : (j + 1) * block])

        return flush(first, last)

    early = terms(0, nz * 3 // 4)
    pg_copy = pltpu.make_async_copy(pg, pg_out, sem)
    pg_copy.start()
    early.start()
    late = terms(nz * 3 // 4, nz)
    late.start()
    for copy in (pg_copy, early, late):
        copy.wait()


def first_kernel(*refs):
    pieces, (w, out, pg_out) = refs[:10], refs[10:13]
    saved, cot, weight, hid, pg_t, pg, term, in_sems, sems = refs[13:]
    block = weight.shape[1] * weight.shape[2]

    def store(i, col, value):
        rows = pl.ds(pl.multiple_of(i * block, block), block)
        term[rows, col : col + value.shape[1]] = value

    def flush(first, last):
        rows = pl.ds(first * block, (last - first) * block)
        return pltpu.make_async_copy(term.at[rows], out.at[rows], sems.at[2 if first else 1])

    weight_copies = [pltpu.make_async_copy(w, weight, sems.at[0])]
    half_products(
        pieces, weight_copies, saved, cot, weight, hid, pg_t, pg, pg_out, store, flush, in_sems, sems.at[3]
    )


def second_kernel(*refs):
    pieces, parts, (out, pg_out) = refs[:10], refs[10:14], refs[14:16]
    saved, cot, weight, hid, pg_t, pg, term, in_sems, w_sems, sems = refs[16:]
    nx, _, part = term.shape[:3]

    def store(i, col, value):
        for j in range(nx):
            term[j, i, :, col : col + value.shape[1]] = value[j * part : (j + 1) * part]

    def flush(first, last):
        at = pl.ds(first, last - first)
        return pltpu.make_async_copy(term.at[:, at], out.at[:, at], sems.at[2 if first else 1])

    weight_copies = []
    for k, piece in enumerate(parts):
        at = (lax.axis_index("x") + (nx - k)) & (nx - 1)
        weight_copies.append(pltpu.make_async_copy(piece, weight.at[:, at], w_sems.at[k]))
    half_products(
        pieces, weight_copies, saved, cot, weight, hid, pg_t, pg, pg_out, store, flush, in_sems, sems.at[3]
    )


def rows_kernel(*refs):
    (pg_a, pg_b, first), parts, (mine_out, theirs_out) = refs[:3], refs[3:7], refs[7:9]
    pg, up, mine, theirs, w_sems, sems = refs[9:]
    width = pg.shape[1] // 2
    a = pltpu.make_async_copy(pg_a, pg.at[:, pl.ds(0, width)], sems.at[0])
    b = pltpu.make_async_copy(pg_b, pg.at[:, pl.ds(width, width)], sems.at[1])
    a.start()
    b.start()
    waits = place_weights(first, parts, up, 0, width, w_sems)
    for copy in (a, b, *waits):
        copy.wait()
    mine_copy = pltpu.make_async_copy(mine, mine_out, sems.at[2])
    theirs_copy = pltpu.make_async_copy(theirs, theirs_out, sems.at[3])
    outputs(pg, mine.shape[0], up, theirs)
    outputs(pg, 0, up, mine, theirs_copy)
    mine_copy.start()
    theirs_copy.wait()
    mine_copy.wait()


def flat_rows(weight, first, count):
    each = weight.shape[1] * weight.shape[2]
    return weight[first // each : (first + count) // each].reshape(count, weight.shape[-1])


def outputs(hidden, first, weight, out, copy=None):
    rows = hidden[pl.ds(first, out.shape[0])]
    for n in range(0, out.shape[1], 512):
        out[:, n : n + 512] = rows_times(rows, flat_rows(weight, n, 512)).astype(BF16)
        if copy is not None and n == 512:
            copy.start()


def ahead_kernel(*refs):
    pieces, first, parts, (mine_out, theirs_out) = refs[:2], refs[2], refs[3:7], refs[7:9]
    rows, up, down, hid, mine, theirs, in_sems, w_sems, sems = refs[9:]
    width = hid.shape[1] // 2
    up_waits = place_weights(first, parts, up, 0, width, w_sems.at[0])
    waits = copies(pieces, rows, in_sems, 0)
    down_waits = place_weights(first, parts, down, width, width, w_sems.at[1])
    for copy in up_waits:
        copy.wait()
    weight = up[...].reshape(-1, 2 * width)
    for t in range(0, rows.shape[0], TILE):
        settle(waits, t + TILE)
        at = pl.ds(t, TILE)
        r = relu_times(rows[at], weight)
        hid[at] = (r * r).astype(BF16)
    for copy in down_waits:
        copy.wait()
    mine_copy = pltpu.make_async_copy(mine, mine_out, sems.at[0])
    theirs_copy = pltpu.make_async_copy(theirs, theirs_out, sems.at[1])
    outputs(hid, mine.shape[0], down, theirs)
    outputs(hid, 0, down, mine, theirs_copy)
    mine_copy.start()
    theirs_copy.wait()
    mine_copy.wait()


def call(kernel, operands, outs, scratch, flops):
    hbm = pl.BlockSpec(memory_space=pltpu.HBM)
    return pl.pallas_call(
        kernel,
        out_shape=[jax.ShapeDtypeStruct(*s) for s in outs],
        in_specs=[hbm] * len(operands),
        out_specs=[hbm] * len(outs),
        scratch_shapes=[pltpu.VMEM(*s) for s in scratch[0]]
        + [pltpu.SemaphoreType.DMA(s) for s in scratch[1]],
        cost_estimate=pl.CostEstimate(flops=flops, bytes_accessed=12 << 20, transcendentals=0),
        compiler_params=pltpu.CompilerParams(vmem_limit_bytes=60 * 1024 * 1024),
    )(*operands)


def products(pieces, later, first, parts):
    rows = sum(p.shape[1] for p in pieces)
    nz, nx, part, cols = first.shape
    depth, width = nz * nx * part, cols // 2
    n = len(pieces)
    flops = 2 * rows * depth * cols
    group, wide = ((rows, depth), BF16), ((rows, cols), BF16)
    split, swapped, flat = (
        ((nz, nx, part, cols), BF16),
        ((nx, nz, part, cols), BF16),
        ((depth, cols), BF16),
    )
    narrow, turned = ((rows, width), BF16), ((width, rows), BF16)
    half = ((rows // 2, depth), BF16)

    def one():
        scratch = (group, group, split, turned, turned, narrow, flat), ((2, n), (4,))
        return call(first_kernel, (*pieces, first), (flat, narrow), scratch, 2 * flops)

    def two():
        scratch = (group, group, split, turned, turned, narrow, swapped), ((2, n), (nx,), (4,))
        return call(second_kernel, (*pieces, *parts), (swapped, narrow), scratch, 2 * flops)

    def row_grad(pg_a, pg_b):
        scratch = (wide, split, half, half), ((nx + 1,), (4,))
        return call(rows_kernel, (pg_a, pg_b, first, *parts), (half, half), scratch, flops)

    def ahead():
        scratch = (group, split, split, wide, half, half), ((2,), (2, nx + 1), (2,))
        return call(ahead_kernel, (*later, first, *parts), (half, half), scratch, 2 * flops)

    return one, two, row_grad, ahead


def body(later_rows, earlier_rows, cotangent, up_weight, down_weight, up_total, down_total):
    n_dev = math.prod(lax.axis_size(a) for a in ALL)
    nz, nx = lax.axis_size("z"), lax.axis_size("x")
    factor = 1.0 / math.sqrt(later_rows.shape[0] * n_dev)
    width = up_weight.shape[1] // 2
    low = jnp.concatenate((up_weight[:, :width], down_weight[:, :width]), axis=1)
    high = jnp.concatenate((up_weight[:, width:], down_weight[:, width:]), axis=1)
    low = gather(low, "x").reshape(-1, low.shape[1])
    low = lax.all_gather(low, "z", axis=0, tiled=True).reshape(nz, nx, *high.shape)
    high = gather(high, "z")
    high = (high, *(shift(high, "x", by) for by in range(1, nx)))
    pieces = gather_tokens((earlier_rows, cotangent))
    later = gather_later(later_rows)
    one, two, row_grad, ahead = products(pieces, later, low, high)
    low_terms, low_pg = one()
    low_terms = lax.psum_scatter(low_terms, "z", scatter_dimension=0, tiled=True)
    high_terms, high_pg = two()
    high_terms = exchange_sum(high_terms, "x").astype(BF16)
    mine, theirs = row_grad(low_pg, high_pg)
    earlier_grad = scatter_tokens(mine, theirs)
    high_terms = exchange_sum(high_terms, "z")
    mine, theirs = ahead()
    later_out = scatter_tokens(mine, theirs)
    low_terms = hop_sum(low_terms.reshape(-1, *up_weight.shape), "x")
    up_term = jnp.concatenate((low_terms[:, :width], high_terms[:, :width]), axis=1)
    down_term = jnp.concatenate((low_terms[:, width:], high_terms[:, width:]), axis=1)
    up_updated = up_total + up_term * factor
    down_updated = down_total + down_term * factor
    return later_out, earlier_grad, up_updated, down_updated


def solution(mesh):
    n_tp = mesh.shape["tp"]
    finer = Mesh(mesh.devices.reshape(8, 4, n_tp // 2, 2), ALL)
    rows, weight = P(ALL, None), P(FS, ("y", "c"))
    return jax.shard_map(
        body,
        mesh=finer,
        in_specs=(rows, rows, rows, weight, weight, weight, weight),
        out_specs=(rows, rows, weight, weight),
        check_vma=False,
    )
```

```python
import math

import jax
import jax.numpy as jnp
from jax import lax
from jax.experimental import pallas as pl
from jax.experimental.pallas import tpu as pltpu
from jax.sharding import Mesh
from jax.sharding import PartitionSpec as P


FS = ("z", "x")
ALL = ("z", "x", "y", "c")
F32 = jnp.float32
BF16 = jnp.bfloat16
TILE = 512


def shift(x, axis, by):
    n = lax.axis_size(axis)
    return lax.ppermute(x, axis, [(i, (i + by) % n) for i in range(n)])


def gather_tokens(arrays):
    own = jnp.stack(arrays)
    half = own.shape[1] // 2
    behind, ahead = shift(own, "y", 1), shift(own, "y", -1)
    far_lo, far_hi = shift(behind[:, :half], "y", 1), shift(ahead[:, half:], "y", -1)
    pieces = (own, behind, ahead, far_lo, far_hi)
    partners = []
    for piece in pieces:
        partners.append(shift(piece, "c", 1))
    return (*pieces, *partners)


def gather_later(own):
    behind, ahead, far = (shift(own, "y", by) for by in (1, -1, 2))
    mine = jnp.concatenate((own, behind, ahead, far), axis=0)[None]
    return mine, shift(mine, "c", 1)


def plus(a, b):
    return (a.astype(F32) + b.astype(F32)).astype(BF16)


def scatter_tokens(mine, partners):
    partners = shift(partners, "c", 1)
    rows = mine.shape[0] // 4
    at = [slice(i * rows, (i + 1) * rows) for i in range(4)]
    behind, ahead, far = (plus(mine[i], partners[i]) for i in at[1:])
    arrived = (shift(ahead, "y", 1), shift(behind, "y", -1), shift(far, "y", 2))
    total = mine[at[0]].astype(F32) + partners[at[0]].astype(F32)
    return sum((a.astype(F32) for a in arrived), total).astype(BF16)


def gather(x, axis):
    n = lax.axis_size(axis)
    return lax.all_to_all(jnp.broadcast_to(x[None], (n, *x.shape)), axis, 0, 0, tiled=True)


def exchange_sum(term, axis):
    tiles = lax.all_to_all(term, axis, 0, 0, tiled=True)
    return jnp.sum(tiles.astype(F32), axis=0)


def hop_sum(term, axis):
    n = lax.axis_size(axis)
    me = lax.axis_index(axis)

    def block(by):
        at = (me + by) & (n - 1)
        start = (at, *(0 for _ in term.shape[1:]))
        part = lax.dynamic_slice(term, start, (1, *term.shape[1:]), allow_negative_indices=False)
        return part[0]

    arrived = [shift(block(by), axis, by) for by in range(1, n)]
    return sum((a.astype(F32) for a in arrived), block(0).astype(F32))


def rows_times(left, right):
    return lax.dot_general(left, right, (((1,), (1,)), ((), ())), preferred_element_type=F32)


def copies(sources, target, sems, index, skip=0):
    waits, row = [], sum(source.shape[1] for source in sources[:skip])
    for i, source in enumerate(sources[skip:], skip):
        rows = source.shape[1]
        copy = pltpu.make_async_copy(source.at[index], target.at[pl.ds(row, rows)], sems.at[i])
        copy.start()
        waits.append((row, copy))
        row += rows
    return waits


def settle(waits, upto):
    while waits and waits[0][0] < upto:
        waits.pop(0)[1].wait()


def relu_times(rows, weight):
    return jnp.maximum(jnp.dot(rows, weight, preferred_element_type=F32), 0.0)


def place_weights(first, parts, target, col, width, sems):
    n = len(parts)
    pairs = [(first.at[:, :, :, pl.ds(col, width)], target.at[:, :, :, pl.ds(0, width)])]
    for k, part in enumerate(parts):
        at = (lax.axis_index("x") + (n - k)) & (n - 1)
        pairs.append((part.at[:, :, pl.ds(col, width)], target.at[:, at, :, pl.ds(width, width)]))
    waits = [pltpu.make_async_copy(a, b, sems.at[i]) for i, (a, b) in enumerate(pairs)]
    for copy in waits:
        copy.start()
    return waits


def half_products(pieces, weight_copies, saved, cot, weight, hid, pg_t, pg, pg_out, store, flush, in_sems, sem):
    for copy in weight_copies:
        copy.start()
    saved_waits = copies(pieces[:5], saved, in_sems.at[0], 0)
    for copy in weight_copies:
        copy.wait()
    cot_waits = copies(pieces[:5], cot, in_sems.at[1], 1)
    saved_waits += copies(pieces, saved, in_sems.at[0], 0, 5)
    cot_waits += copies(pieces, cot, in_sems.at[1], 1, 5)
    width = hid.shape[0]
    both = weight[...].reshape(-1, 2 * width)
    for t in range(0, saved.shape[0], TILE):
        at = pl.ds(t, TILE)
        settle(saved_waits, t + TILE)
        r = relu_times(saved[at], both[:, :width])
        hid[:, at] = (r * r).astype(BF16).T
        settle(cot_waits, t + TILE)
        grad = jnp.dot(cot[at], both[:, width:], preferred_element_type=F32)
        piece = (2.0 * r * grad).astype(BF16)
        pg[at] = piece
        pg_t[:, at] = piece.T
    nz, block = weight.shape[0], weight.shape[1] * weight.shape[2]

    def terms(first, last):
        @pl.loop(first, last, step=2)
        def _(i):
            at = pl.ds(pl.multiple_of(i * block, 2 * block), 2 * block)
            up = jnp.dot(pg_t[...], saved[:, at], preferred_element_type=F32).astype(BF16).T
            down = jnp.dot(hid[...], cot[:, at], preferred_element_type=F32).astype(BF16).T
            for j in range(2):
                store(i + j, 0, up[j * block : (j + 1) * block])
                store(i + j, width, down[j * block : (j + 1) * block])

        return flush(first, last)

    early = terms(0, nz * 3 // 4)
    pg_copy = pltpu.make_async_copy(pg, pg_out, sem)
    pg_copy.start()
    early.start()
    late = terms(nz * 3 // 4, nz)
    late.start()
    for copy in (pg_copy, early, late):
        copy.wait()


def first_kernel(*refs):
    pieces, (w, out, pg_out) = refs[:10], refs[10:13]
    saved, cot, weight, hid, pg_t, pg, term, in_sems, sems = refs[13:]
    block = weight.shape[1] * weight.shape[2]

    def store(i, col, value):
        rows = pl.ds(pl.multiple_of(i * block, block), block)
        term[rows, col : col + value.shape[1]] = value

    def flush(first, last):
        rows = pl.ds(first * block, (last - first) * block)
        return pltpu.make_async_copy(term.at[rows], out.at[rows], sems.at[2 if first else 1])

    weight_copies = [pltpu.make_async_copy(w, weight, sems.at[0])]
    half_products(
        pieces, weight_copies, saved, cot, weight, hid, pg_t, pg, pg_out, store, flush, in_sems, sems.at[3]
    )


def second_kernel(*refs):
    pieces, parts, (out, pg_out) = refs[:10], refs[10:14], refs[14:16]
    saved, cot, weight, hid, pg_t, pg, term, in_sems, w_sems, sems = refs[16:]
    nx, _, part = term.shape[:3]

    def store(i, col, value):
        for j in range(nx):
            term[j, i, :, col : col + value.shape[1]] = value[j * part : (j + 1) * part]

    def flush(first, last):
        at = pl.ds(first, last - first)
        return pltpu.make_async_copy(term.at[:, at], out.at[:, at], sems.at[2 if first else 1])

    weight_copies = []
    for k, piece in enumerate(parts):
        at = (lax.axis_index("x") + (nx - k)) & (nx - 1)
        weight_copies.append(pltpu.make_async_copy(piece, weight.at[:, at], w_sems.at[k]))
    half_products(
        pieces, weight_copies, saved, cot, weight, hid, pg_t, pg, pg_out, store, flush, in_sems, sems.at[3]
    )


def rows_kernel(*refs):
    (pg_a, pg_b, first), parts, (mine_out, theirs_out) = refs[:3], refs[3:7], refs[7:9]
    pg, up, mine, theirs, w_sems, sems = refs[9:]
    width = pg.shape[1] // 2
    a = pltpu.make_async_copy(pg_a, pg.at[:, pl.ds(0, width)], sems.at[0])
    b = pltpu.make_async_copy(pg_b, pg.at[:, pl.ds(width, width)], sems.at[1])
    a.start()
    b.start()
    waits = place_weights(first, parts, up, 0, width, w_sems)
    for copy in (a, b, *waits):
        copy.wait()
    mine_copy = pltpu.make_async_copy(mine, mine_out, sems.at[2])
    theirs_copy = pltpu.make_async_copy(theirs, theirs_out, sems.at[3])
    outputs(pg, mine.shape[0], up, theirs)
    outputs(pg, 0, up, mine, theirs_copy)
    mine_copy.start()
    theirs_copy.wait()
    mine_copy.wait()


def flat_rows(weight, first, count):
    each = weight.shape[1] * weight.shape[2]
    return weight[first // each : (first + count) // each].reshape(count, weight.shape[-1])


def outputs(hidden, first, weight, out, copy=None):
    rows = hidden[pl.ds(first, out.shape[0])]
    for n in range(0, out.shape[1], 512):
        out[:, n : n + 512] = rows_times(rows, flat_rows(weight, n, 512)).astype(BF16)
        if copy is not None and n == 512:
            copy.start()


def ahead_kernel(*refs):
    pieces, first, parts, (mine_out, theirs_out) = refs[:2], refs[2], refs[3:7], refs[7:9]
    rows, up, down, hid, mine, theirs, in_sems, w_sems, sems = refs[9:]
    width = hid.shape[1] // 2
    up_waits = place_weights(first, parts, up, 0, width, w_sems.at[0])
    waits = copies(pieces, rows, in_sems, 0)
    down_waits = place_weights(first, parts, down, width, width, w_sems.at[1])
    for copy in up_waits:
        copy.wait()
    weight = up[...].reshape(-1, 2 * width)
    for t in range(0, rows.shape[0], TILE):
        settle(waits, t + TILE)
        at = pl.ds(t, TILE)
        r = relu_times(rows[at], weight)
        hid[at] = (r * r).astype(BF16)
    for copy in down_waits:
        copy.wait()
    mine_copy = pltpu.make_async_copy(mine, mine_out, sems.at[0])
    theirs_copy = pltpu.make_async_copy(theirs, theirs_out, sems.at[1])
    outputs(hid, mine.shape[0], down, theirs)
    outputs(hid, 0, down, mine, theirs_copy)
    mine_copy.start()
    theirs_copy.wait()
    mine_copy.wait()


def call(kernel, operands, outs, scratch, flops):
    hbm = pl.BlockSpec(memory_space=pltpu.HBM)
    return pl.pallas_call(
        kernel,
        out_shape=[jax.ShapeDtypeStruct(*s) for s in outs],
        in_specs=[hbm] * len(operands),
        out_specs=[hbm] * len(outs),
        scratch_shapes=[pltpu.VMEM(*s) for s in scratch[0]]
        + [pltpu.SemaphoreType.DMA(s) for s in scratch[1]],
        cost_estimate=pl.CostEstimate(flops=flops, bytes_accessed=12 << 20, transcendentals=0),
        compiler_params=pltpu.CompilerParams(vmem_limit_bytes=60 * 1024 * 1024),
    )(*operands)


def products(pieces, later, first, parts):
    rows = sum(p.shape[1] for p in pieces)
    nz, nx, part, cols = first.shape
    depth, width = nz * nx * part, cols // 2
    n = len(pieces)
    flops = 2 * rows * depth * cols
    group, wide = ((rows, depth), BF16), ((rows, cols), BF16)
    split, swapped, flat = (
        ((nz, nx, part, cols), BF16),
        ((nx, nz, part, cols), BF16),
        ((depth, cols), BF16),
    )
    narrow, turned = ((rows, width), BF16), ((width, rows), BF16)
    half = ((rows // 2, depth), BF16)

    def one():
        scratch = (group, group, split, turned, turned, narrow, flat), ((2, n), (4,))
        return call(first_kernel, (*pieces, first), (flat, narrow), scratch, 2 * flops)

    def two():
        scratch = (group, group, split, turned, turned, narrow, swapped), ((2, n), (nx,), (4,))
        return call(second_kernel, (*pieces, *parts), (swapped, narrow), scratch, 2 * flops)

    def row_grad(pg_a, pg_b):
        scratch = (wide, split, half, half), ((nx + 1,), (4,))
        return call(rows_kernel, (pg_a, pg_b, first, *parts), (half, half), scratch, flops)

    def ahead():
        scratch = (group, split, split, wide, half, half), ((2,), (2, nx + 1), (2,))
        return call(ahead_kernel, (*later, first, *parts), (half, half), scratch, 2 * flops)

    return one, two, row_grad, ahead


def body(later_rows, earlier_rows, cotangent, up_weight, down_weight, up_total, down_total):
    n_dev = math.prod(lax.axis_size(a) for a in ALL)
    nz, nx = lax.axis_size("z"), lax.axis_size("x")
    factor = 1.0 / math.sqrt(later_rows.shape[0] * n_dev)
    width = up_weight.shape[1] // 2
    low = jnp.concatenate((up_weight[:, :width], down_weight[:, :width]), axis=1)
    high = jnp.concatenate((up_weight[:, width:], down_weight[:, width:]), axis=1)
    low = gather(low, "x").reshape(-1, low.shape[1])
    low = lax.all_gather(low, "z", axis=0, tiled=True).reshape(nz, nx, *high.shape)
    high = gather(high, "z")
    high = (high, *(shift(high, "x", by) for by in range(1, nx)))
    pieces = gather_tokens((earlier_rows, cotangent))
    later = gather_later(later_rows)
    one, two, row_grad, ahead = products(pieces, later, low, high)
    low_terms, low_pg = one()
    low_terms = lax.psum_scatter(low_terms, "z", scatter_dimension=0, tiled=True)
    high_terms, high_pg = two()
    high_terms = exchange_sum(high_terms, "x").astype(BF16)
    mine, theirs = row_grad(low_pg, high_pg)
    earlier_grad = scatter_tokens(mine, theirs)
    high_terms = exchange_sum(high_terms, "z")
    mine, theirs = ahead()
    later_out = scatter_tokens(mine, theirs)
    low_terms = hop_sum(low_terms.reshape(-1, *up_weight.shape), "x")
    up_term = jnp.concatenate((low_terms[:, :width], high_terms[:, :width]), axis=1)
    down_term = jnp.concatenate((low_terms[:, width:], high_terms[:, width:]), axis=1)
    up_updated = up_total + up_term * factor
    down_updated = down_total + down_term * factor
    return later_out, earlier_grad, up_updated, down_updated


def solution(mesh):
    n_tp = mesh.shape["tp"]
    finer = Mesh(mesh.devices.reshape(8, 4, n_tp // 2, 2), ALL)
    rows, weight = P(ALL, None), P(FS, ("y", "c"))
    return jax.shard_map(
        body,
        mesh=finer,
        in_specs=(rows, rows, rows, weight, weight, weight, weight),
        out_specs=(rows, rows, weight, weight),
        check_vma=False,
    )
```
